32 devices in a mesh: grp: 2 (over y), sp: 4 (over z), tp: 4 (over x, core).
Axes of the slice: x: 2, y: 2, z: 4, core: 2. Of those that a mesh axis runs over, the one named last changes fastest.
Arguments:
- window_query: bfloat16 [2560, 2048], P(('grp', 'sp'), 'tp'), parts along dimension 0, may hold values from -24 to 24
- window_key: bfloat16 [2560, 1024], P(('grp', 'sp'), 'tp'), parts along dimension 0, may hold values from -24 to 24
- window_value: bfloat16 [2560, 1024], P(('grp', 'sp'), 'tp'), parts along dimension 0, may hold values from -6 to 6
- grid_query: bfloat16 [2560, 2048], P(('grp', 'sp'), 'tp'), parts along dimension 0, may hold values from -10 to 10
- grid_key: bfloat16 [2560, 1024], P(('grp', 'sp'), 'tp'), parts along dimension 0, may hold values from -10 to 10
- grid_value: bfloat16 [2560, 1024], P(('grp', 'sp'), 'tp'), parts along dimension 0, may hold values from -6 to 6
- sink_logit: float32 [16], P('tp'), may hold values from 1 to 6
- query_gain: float32 [128], replicated, may hold values from 0.8 to 6
- key_gain: float32 [128], replicated, may hold values from 0.8 to 6
- window_weights: bfloat16 [2048, 4096], P('tp'), may hold values from -0.59765625 to 0.59765625
- grid_weights: bfloat16 [2048, 4096], P('tp'), may hold values from -0.59765625 to 0.59765625
Outputs:
- merged: bfloat16 [2560, 4096], P(('grp', 'sp', 'tp')), parts along dimension 0
The draws below stay inside these ranges and needn't reach their ends.
There are 2 independent parts, one for each index of `grp`. The reference program is written for one: setup_inputs(seed, part) draws one part's arguments, and reference() takes and returns one part's arrays. A program takes and returns all parts, laid end to end along the dimension named above; an argument that names none is the same for every part. Nothing has to cross between parts.
All inputs are finite; a program needn't handle non-finite values.
Results may differ from the reference program's by a relative error of at most 0.014.
The reference program's roundings to bfloat16 on the way count: a program that leaves them out, or rounds other values in their place, can miss the bound.
Values may be sent and summed in bfloat16 or wider, within the bound.
A program may use at most 64 MiB of HBM per device.

```python
import jax
import jax.numpy as jnp
from jax import lax

D = 4096
HEAD = 128
QH_A = 16
KVH_A = 8
QH_B = 16
KVH_B = 8
WINDOW = 128
GRID_W = 64
TOKENS = 1280
N_SP = 4
N_TP = 4


def pair_window(key):
    base = jax.random.fold_in(key, 101)
    key_query, key_key = jax.random.split(base, 2)
    queries = jnp.clip(jax.random.normal(key_query, (TOKENS, QH_A * HEAD), jnp.float32), -6.0, 6.0)
    keys = jnp.clip(jax.random.normal(key_key, (TOKENS, KVH_A * HEAD), jnp.float32), -6.0, 6.0)
    return (queries, keys)


def pair_grid(key):
    base = jax.random.fold_in(key, 202)
    key_query, key_key = jax.random.split(base, 2)
    queries = jnp.clip(jax.random.normal(key_query, (TOKENS, QH_B * HEAD), jnp.float32), -6.0, 6.0)
    keys = jnp.clip(jax.random.normal(key_key, (TOKENS, KVH_B * HEAD), jnp.float32), -6.0, 6.0)
    return (queries, keys)


def grid_gain(key, salt):
    base = jax.random.fold_in(key, salt)
    return 1.5 + 0.27 * jnp.clip(jax.random.normal(base, (HEAD,), jnp.float32), -2.5, 2.5)


def draw_window_query(key, part):
    return pair_window(key)[0].astype(jnp.bfloat16)


def draw_window_key(key, part):
    return pair_window(key)[1].astype(jnp.bfloat16)


def draw_grid_query(key, part):
    return pair_grid(key)[0].astype(jnp.bfloat16)


def draw_grid_key(key, part):
    return pair_grid(key)[1].astype(jnp.bfloat16)


def draw_query_gain(key, part):
    return grid_gain(key, 303)


def draw_key_gain(key, part):
    return grid_gain(key, 404)


def steps_of(rng, dims, shards, low, high):
    def one(dim, blocks):
        heights = jax.random.uniform(jax.random.fold_in(jax.random.fold_in(rng, 6), dim), (blocks,), jnp.float32, low / len(shards), high / len(shards))
        return jnp.repeat(jnp.exp(heights), dims[dim] // blocks).reshape((-1,) + (1,) * (len(dims) - dim - 1))

    loudness = one(*shards[0])
    for cut in shards[1:]:
        loudness = loudness * one(*cut)
    return loudness


def noise(own_key, extent, scale, most, cuts=(), held_as=jnp.bfloat16):
    entries = scale * jax.random.normal(own_key, extent, jnp.float32)
    if cuts:
        entries = entries * steps_of(own_key, extent, cuts, -0.22, 0.18)
    return jnp.clip(entries, -most, most).astype(held_as)


def setup_inputs(seed: int = 0, part: int = 0) -> dict:
    key_list = jax.random.split(jax.random.key(seed), 12)
    part_keys = jax.random.split(jax.random.fold_in(key_list[11], part), 12)
    return {
        "window_query": draw_window_query(jax.random.fold_in(jax.random.fold_in(key_list[11], part), 71), part),
        "window_key": draw_window_key(jax.random.fold_in(jax.random.fold_in(key_list[11], part), 71), part),
        "window_value": noise(part_keys[2], (TOKENS, KVH_A * HEAD), 1.0, 6.0, ((0, 4), (1, 4))),
        "grid_query": draw_grid_query(jax.random.fold_in(jax.random.fold_in(key_list[11], part), 71), part),
        "grid_key": draw_grid_key(jax.random.fold_in(jax.random.fold_in(key_list[11], part), 71), part),
        "grid_value": noise(part_keys[5], (TOKENS, KVH_B * HEAD), 1.0, 6.0, ((0, 4), (1, 4))),
        "sink_logit": jnp.clip(1.0 + 5.0 * jax.random.uniform(key_list[6], (QH_A,), jnp.float32) ** steps_of(key_list[6], (QH_A,), ((0, 4),), -0.2, 0.2), 1.0, 6.0),
        "query_gain": draw_query_gain(jax.random.fold_in(key_list[11], 71), part),
        "key_gain": draw_key_gain(jax.random.fold_in(key_list[11], 71), part),
        "window_weights": noise(key_list[9], (QH_A * HEAD, D), 0.1, 0.59765625, ((0, 4),)),
        "grid_weights": noise(key_list[10], (QH_B * HEAD, D), 0.1, 0.59765625, ((0, 4),)),
    }


THETA = 10000.0
NEGATIVE = -1e+30
EPSILON = 1e-06

def turn_section(values, places):
    width = values.shape[-1]
    half_width = width // 2
    frequency = THETA ** (-jnp.arange(0, width, 2, dtype=jnp.float32) / width)
    angles = places[:, None] * frequency[None, :]
    cosine = jnp.cos(angles)[:, None, :]
    sine_part = jnp.sin(angles)[:, None, :]
    first_half = values[..., :half_width]
    second_half = values[..., half_width:]
    return jnp.concatenate([first_half * cosine - second_half * sine_part, second_half * cosine + first_half * sine_part], axis=-1)

def normed_turn(values, gain, places):
    count_rows = values.shape[0]
    shaped = values.astype(jnp.float32).reshape(count_rows, -1, HEAD)
    scaled = shaped * lax.rsqrt(lax.optimization_barrier(jnp.mean(shaped * shaped, axis=-1, keepdims=True)) + EPSILON)
    scaled = scaled * gain.astype(jnp.float32)
    grid_row = (places // GRID_W).astype(jnp.float32)
    grid_col = (places % GRID_W).astype(jnp.float32)
    section = HEAD // 2
    turned = jnp.concatenate([turn_section(scaled[..., :section], grid_row), turn_section(scaled[..., section:], grid_col)], axis=-1)
    return turned.astype(jnp.bfloat16)

def window_attend(queries, keys_pad, values_pad, slopes, sink_logits, offset, total_rows):
    query_rows = queries.shape[0]
    block_span = WINDOW // 2
    blocks = query_rows // block_span
    key_heads = keys_pad.shape[1] // HEAD
    group_size = queries.shape[1] // keys_pad.shape[1]
    query_blocks = queries.astype(jnp.float32).reshape(blocks, block_span, key_heads, group_size, HEAD)
    key_blocks = keys_pad.astype(jnp.float32).reshape(blocks + 4, block_span, key_heads, HEAD)
    value_blocks = values_pad.astype(jnp.float32).reshape(blocks + 4, block_span, key_heads, HEAD)
    key_window = jnp.concatenate([key_blocks[block_shift:block_shift + blocks] for block_shift in range(5)], axis=1)
    value_window = jnp.concatenate([value_blocks[block_shift:block_shift + blocks] for block_shift in range(5)], axis=1)
    scores = jnp.einsum('nqkgd,nskd->kgnqs', query_blocks, key_window) * HEAD ** (-0.5)
    query_place = offset + jnp.arange(query_rows, dtype=jnp.int32).reshape(blocks, block_span, 1)
    key_place = offset - WINDOW + block_span * jnp.arange(blocks, dtype=jnp.int32)[:, None, None] + jnp.arange(5 * block_span, dtype=jnp.int32)[None, None, :]
    distance = jnp.abs(key_place - query_place)
    inside = (distance <= WINDOW) & (key_place >= 0) & (key_place < total_rows)
    slope_grid = slopes.reshape(key_heads, group_size, 1, 1, 1)
    sink_grid = sink_logits.astype(jnp.float32).reshape(key_heads, group_size, 1, 1)
    scores = jnp.where(inside, scores - slope_grid * distance.astype(jnp.float32), NEGATIVE)
    highest = jnp.maximum(lax.optimization_barrier(jnp.max(scores, axis=-1)), sink_grid)
    raised = jnp.exp(scores - highest[..., None])
    denominator = lax.optimization_barrier(jnp.sum(raised, axis=-1)) + jnp.exp(sink_grid - highest)
    weights = lax.optimization_barrier((raised / denominator[..., None]).astype(jnp.bfloat16))
    attended = jnp.einsum('kgnqs,nskd->nqkgd', weights.astype(jnp.float32), value_window)
    return attended.astype(jnp.bfloat16).reshape(query_rows, -1)

def reference(window_query, window_key, window_value, grid_query, grid_key, grid_value, sink_logit, query_gain, key_gain, window_weights, grid_weights):
    total_rows = window_query.shape[0]
    places = jnp.arange(total_rows, dtype=jnp.int32)
    slopes = 2.0 ** (-8.0 * jnp.arange(1, QH_A + 1, dtype=jnp.float32) / QH_A)
    padding = ((WINDOW, WINDOW), (0, 0))
    window_out = window_attend(window_query, jnp.pad(window_key, padding), jnp.pad(window_value, padding), slopes, sink_logit, 0, total_rows)
    group_size = QH_B // KVH_B
    turned_q = lax.optimization_barrier(normed_turn(grid_query, query_gain, places))
    turned_q = turned_q.astype(jnp.float32).reshape(total_rows, KVH_B, group_size, HEAD)
    turned_k = lax.optimization_barrier(normed_turn(grid_key, key_gain, places))
    key_pieces = turned_k.astype(jnp.float32).reshape(N_SP, total_rows // N_SP, KVH_B, HEAD)
    value_pieces = grid_value.astype(jnp.float32).reshape(N_SP, total_rows // N_SP, KVH_B, HEAD)

    def absorb(carry, block_pair):
        highest, summed, gathered = carry
        key_block, value_block = block_pair
        scores = jnp.einsum('tkgd,skd->kgts', turned_q, key_block) * HEAD ** (-0.5)
        raised_top = jnp.maximum(highest, lax.optimization_barrier(jnp.max(scores, axis=-1)))
        fading = jnp.exp(highest - raised_top)
        raised = jnp.exp(scores - raised_top[..., None])
        summed = summed * fading + lax.optimization_barrier(jnp.sum(raised, axis=-1))
        rounded = lax.optimization_barrier(raised.astype(jnp.bfloat16)).astype(jnp.float32)
        gathered = gathered * fading[..., None] + jnp.einsum('kgts,skd->kgtd', rounded, value_block)
        return ((raised_top, summed, gathered), None)
    start_carry = (jnp.full((KVH_B, group_size, total_rows), NEGATIVE, jnp.float32), jnp.zeros((KVH_B, group_size, total_rows), jnp.float32), jnp.zeros((KVH_B, group_size, total_rows, HEAD), jnp.float32))
    final_carry, _ = lax.scan(absorb, start_carry, (key_pieces, value_pieces))
    grid_out = (final_carry[2] / final_carry[1][..., None]).astype(jnp.bfloat16)
    width_a = QH_A // N_TP * HEAD
    heads_b = KVH_B // N_TP
    shaped_b = grid_weights.reshape(KVH_B, group_size, HEAD, D)

    def group_term(running, group_index):
        part_a = lax.dynamic_slice_in_dim(window_out, group_index * width_a, width_a, 1)
        rows_a = lax.dynamic_slice_in_dim(window_weights, group_index * width_a, width_a, 0)
        part_b = lax.dynamic_slice_in_dim(grid_out, group_index * heads_b, heads_b, 0)
        rows_b = lax.dynamic_slice_in_dim(shaped_b, group_index * heads_b, heads_b, 0)
        partial_term = jnp.dot(part_a, rows_a, preferred_element_type=jnp.float32)
        partial_term = partial_term + jnp.einsum('kgtd,kgdo->to', part_b.astype(jnp.float32), rows_b.astype(jnp.float32))
        partial_term = lax.optimization_barrier(partial_term.astype(jnp.bfloat16)).astype(jnp.float32)
        return (running + partial_term, None)
    merged, _ = lax.scan(group_term, jnp.zeros((total_rows, D), jnp.float32), jnp.arange(N_TP, dtype=jnp.int32))
    return merged.astype(jnp.bfloat16)
```

```python
import functools
import math

import jax
import jax.numpy as jnp
from jax import lax
from jax.experimental import pallas as pl
from jax.experimental.pallas import tpu as pltpu
from jax.sharding import PartitionSpec as P

HEAD = 128
QH_A = 16
WINDOW = 128
GRID_W = 64
THETA = 10000.0
NEGATIVE = -1e30
EPSILON = 1e-06
MESH = pl.DeviceIdType.MESH
F32 = jnp.float32
BF16 = jnp.bfloat16


def dot_nt(a, b):
    return lax.dot_general(a, b, (((1,), (1,)), ((), ())), preferred_element_type=F32)


def dot_tn(a, b):
    return lax.dot_general(a, b, (((0,), (0,)), ((), ())), preferred_element_type=F32)


def kernel(
    n, n_tp, rows, kvh, group, chunks,
    wq_hbm, wk_hbm, wv_hbm, gq_hbm, gk_hbm, gv_hbm, sink_hbm, qgain_hbm, kgain_hbm, ww_hbm, gw_hbm,
    out_ref,
    sink_ref, qgain_ref, kgain_ref, qw, wkv, qraw, kraw, qg, kvbuf, ww, gw, cosine, sine, top, total, acc, attn, proj, pbuf, dbuf, sbuf, rbuf, own,
    lsem, gsend, grecv, hsend, hrecv, dsend, drecv, xsend, xrecv,
):
    me = lax.axis_index("sp")
    t = lax.axis_index("tp")
    core = lax.rem(t, 2)
    x = t // 2
    n_x = n_tp // 2
    partner = x * 2 + 1 - core
    out_rows = rows // n_tp
    width = ww.shape[1] // chunks
    span = group * rows
    has_left = me > 0
    has_right = me < n - 1

    barrier = pltpu.get_barrier_semaphore()

    def greet(device):
        pl.semaphore_signal(barrier, inc=1, device_id=device, device_id_type=MESH)

    @pl.when(has_left)
    def _():
        greet({"sp": me - 1})

    @pl.when(has_right)
    def _():
        greet({"sp": me + 1})

    greet({"tp": partner})
    for dx in range(1, n_x):
        greet({"tp": lax.rem(x + dx, n_x) * 2 + core})

    loads = []

    def load(src, dst):
        copy = pltpu.make_async_copy(src, dst, lsem.at[len(loads)])
        copy.start()
        loads.append(copy)
        return copy

    def head_cols(h):
        return slice(h * HEAD, (h + 1) * HEAD)

    v_loads = [load(gv_hbm.at[:, head_cols(g)], kvbuf.at[me, g, 1]) for g in range(kvh)]
    k_loads = [load(gk_hbm.at[:, head_cols(g)], kraw.at[g]) for g in range(kvh)]
    kgain_load = load(kgain_hbm, kgain_ref)
    qgain_load = load(qgain_hbm, qgain_ref)
    sink_load = load(sink_hbm, sink_ref)
    w_loads = []
    for g in range(kvh):
        w_loads.append(load(wk_hbm.at[:, head_cols(g)], wkv.at[g, 0, WINDOW : WINDOW + rows]))
        w_loads.append(load(wv_hbm.at[:, head_cols(g)], wkv.at[g, 1, WINDOW : WINDOW + rows]))
    q_loads = []
    for g in range(kvh):
        for u in range(group):
            q_loads.append(load(gq_hbm.at[:, head_cols(g * group + u)], qraw.at[g, u * rows : (u + 1) * rows]))
    wq_loads = []
    for g in range(kvh):
        for u in range(group):
            wq_loads.append(load(wq_hbm.at[:, head_cols(g * group + u)], qw.at[g, u * rows : (u + 1) * rows]))
    ww_load = load(ww_hbm, ww)
    gw_load = load(gw_hbm, gw)

    section = HEAD // 2
    half = section // 2

    def angles(row_place, column_place, shape):
        lane = lax.broadcasted_iota(jnp.int32, shape, 1)
        frequency = jnp.exp(jnp.bitwise_and(lane, half - 1).astype(F32) * (-2.0 * math.log(THETA) / section))
        return jnp.where(lane < section, row_place, column_place).astype(F32) * frequency

    def signed_sine(angle):
        low = jnp.bitwise_and(lax.broadcasted_iota(jnp.int32, angle.shape, 1), section - 1) < half
        return jnp.where(low, -jnp.sin(angle), jnp.sin(angle))

    def make_tables():
        if rows % GRID_W:
            place = me * rows + lax.broadcasted_iota(jnp.int32, (rows, HEAD), 0)
            angle = angles(place // GRID_W, lax.rem(place, GRID_W), (rows, HEAD))
            cosine[...] = jnp.cos(angle)
            sine[...] = signed_sine(angle)
            return
        lines = rows // GRID_W
        shape = (-(-lines // 8) * 8, HEAD)
        line = me * lines + lax.broadcasted_iota(jnp.int32, shape, 0)
        row_angle = angles(line, line, shape)
        column = lax.broadcasted_iota(jnp.int32, (GRID_W, HEAD), 0)
        column_angle = angles(column, column, (GRID_W, HEAD))
        by_row = lax.broadcasted_iota(jnp.int32, (GRID_W, HEAD), 1) < section
        for table, of in ((cosine, jnp.cos), (sine, signed_sine)):
            per_row, per_column = of(row_angle), of(column_angle)
            for r in range(lines):
                table[r * GRID_W : (r + 1) * GRID_W] = jnp.where(by_row, per_row[r : r + 1], per_column)

    def turn(values, gain):
        v = values.astype(F32)
        v = v * lax.rsqrt(jnp.mean(v * v, axis=1, keepdims=True) + EPSILON) * gain
        first = lax.broadcasted_iota(jnp.int32, v.shape, 1)
        other = jnp.where(
            jnp.bitwise_and(first, section - 1) < half,
            pltpu.roll(v, HEAD - half, 1),
            pltpu.roll(v, half, 1),
        )
        return (v * cosine[...] + other * sine[...]).astype(BF16)

    def block_copy(source, g, part, direction):
        return pltpu.make_async_remote_copy(
            src_ref=kvbuf.at[source, g, part],
            dst_ref=kvbuf.at[source, g, part],
            send_sem=gsend.at[direction, source, g, part],
            recv_sem=grecv.at[source, g, part],
            device_id={"sp": me + 1 if direction == 0 else me - 1},
            device_id_type=MESH,
        )

    def spread(g, part):
        @pl.when(has_right)
        def _():
            block_copy(me, g, part, 0).start()

        @pl.when(has_left)
        def _():
            block_copy(me, g, part, 1).start()

    def halo_copy(direction):
        source = rows if direction == 0 else WINDOW
        target = 0 if direction == 0 else WINDOW + rows
        return pltpu.make_async_remote_copy(
            src_ref=wkv.at[:, :, source : source + WINDOW],
            dst_ref=wkv.at[:, :, target : target + WINDOW],
            send_sem=hsend.at[direction],
            recv_sem=hrecv.at[direction],
            device_id={"sp": me + 1 if direction == 0 else me - 1},
            device_id_type=MESH,
        )

    for copy in v_loads:
        copy.wait()
    pl.semaphore_wait(barrier, has_left.astype(jnp.int32) + has_right.astype(jnp.int32) + n_x)
    for g in range(kvh):
        spread(g, 1)

    make_tables()
    kgain_load.wait()
    for g in range(kvh):
        k_loads[g].wait()
        kvbuf[me, g, 0] = turn(kraw[g], kgain_ref[...])
        spread(g, 0)

    for copy in w_loads:
        copy.wait()

    @pl.when(has_right)
    def _():
        halo_copy(0).start()

    @pl.when(has_left)
    def _():
        halo_copy(1).start()

    @pl.when(jnp.logical_not(has_left))
    def _():
        wkv[:, :, 0:WINDOW] = jnp.zeros((kvh, 2, WINDOW, HEAD), BF16)

    @pl.when(jnp.logical_not(has_right))
    def _():
        wkv[:, :, WINDOW + rows :] = jnp.zeros((kvh, 2, WINDOW, HEAD), BF16)

    qgain_load.wait()
    for copy in q_loads:
        copy.wait()
    for g in range(kvh):
        for u in range(group):
            part = slice(u * rows, (u + 1) * rows)
            qg[g, part] = turn(qraw[g, part], qgain_ref[...])

    scale = HEAD ** (-0.5)

    def absorb(source, g, first=False):
        scores = dot_nt(kvbuf[source, g, 0], qg[g]) * scale
        block_top = jnp.max(scores, axis=0, keepdims=True)
        if first:
            raised = jnp.exp(scores - block_top)
            top[g] = block_top
            total[g] = jnp.sum(raised, axis=0, keepdims=True)
            acc[g] = dot_tn(kvbuf[source, g, 1], raised.astype(BF16))
        else:
            before = top[g]
            new_top = jnp.maximum(before, block_top)
            fading = jnp.exp(before - new_top)
            raised = jnp.exp(scores - new_top)
            top[g] = new_top
            total[g] = total[g] * fading + jnp.sum(raised, axis=0, keepdims=True)
            acc[g] = acc[g] * fading + dot_tn(kvbuf[source, g, 1], raised.astype(BF16))

    for g in range(kvh):
        absorb(me, g, True)

    def relay(d):
        for part in (1, 0):
            for g in range(kvh):
                @pl.when(me - d >= 0)
                def _():
                    block_copy(me - d, g, part, 0).wait_recv()

                    @pl.when(has_right)
                    def _():
                        block_copy(me - d, g, part, 0).start()

                @pl.when(me + d < n)
                def _():
                    block_copy(me + d, g, part, 1).wait_recv()

                    @pl.when(has_left)
                    def _():
                        block_copy(me + d, g, part, 1).start()

                if part == 0:
                    @pl.when(me - d >= 0)
                    def _():
                        absorb(me - d, g)

                    @pl.when(me + d < n)
                    def _():
                        absorb(me + d, g)

    def put_heads(base, g, value):
        turned = jnp.transpose(value).astype(BF16)
        for u in range(group):
            attn[:, base + (g * group + u) * HEAD : base + (g * group + u + 1) * HEAD] = turned[u * rows : (u + 1) * rows]

    heads_width = kvh * group * HEAD

    def windowed():
        sink_load.wait()
        for copy in wq_loads:
            copy.wait()

        @pl.when(has_left)
        def _():
            halo_copy(0).wait_recv()

        @pl.when(has_right)
        def _():
            halo_copy(1).wait_recv()

        padded = rows + 2 * WINDOW
        key_at = lax.broadcasted_iota(jnp.int32, (padded, span), 0) - WINDOW
        column = lax.broadcasted_iota(jnp.int32, (padded, span), 1)
        distance = jnp.abs(key_at - lax.rem(column, rows))
        key_place = me * rows + key_at
        inside = (distance <= WINDOW) & (key_place >= 0) & (key_place < n * rows)
        far = distance.astype(F32)
        member = lax.broadcasted_iota(jnp.int32, (1, span), 1) // rows
        for g in range(kvh):
            head = (t * (kvh * group) + g * group + 1 + member).astype(F32)
            slope = jnp.exp2(head * (-8.0 / QH_A))
            sink = jnp.zeros((1, span), F32)
            for u in range(group):
                sink = jnp.where(member == u, sink_ref[g * group + u], sink)
            scores = dot_nt(wkv[g, 0], qw[g]) * scale
            scores = jnp.where(inside, scores - slope * far, NEGATIVE)
            highest = jnp.maximum(jnp.max(scores, axis=0, keepdims=True), sink)
            raised = jnp.exp(scores - highest)
            bottom = jnp.sum(raised, axis=0, keepdims=True) + jnp.exp(sink - highest)
            weights = (raised * (1.0 / bottom)).astype(BF16)
            put_heads(0, g, dot_tn(wkv[g, 1], weights))
        ww_load.wait()
        for j in range(chunks):
            cols = slice(j * width, (j + 1) * width)
            proj[:, cols] = jnp.dot(attn[:, :heads_width], ww[:, cols], preferred_element_type=F32)

    if n > 1:
        relay(1)
    windowed()
    if n <= 4:
        for d in range(2, n):
            relay(d)
    else:
        def relay_step(d, carry):
            relay(d)
            return carry

        lax.fori_loop(2, n, relay_step, 0)

    for g in range(kvh):
        put_heads(heads_width, g, acc[g] * (1.0 / total[g]))
    gw_load.wait()

    def pair_copy(j):
        return pltpu.make_async_remote_copy(
            src_ref=pbuf.at[j, 1 - core],
            dst_ref=dbuf.at[j],
            send_sem=dsend.at[j],
            recv_sem=drecv.at[j],
            device_id={"tp": partner},
            device_id_type=MESH,
        )

    def cross_copy(j, dx):
        return pltpu.make_async_remote_copy(
            src_ref=sbuf.at[j, dx - 1],
            dst_ref=rbuf.at[j, dx - 1],
            send_sem=xsend.at[j, dx - 1],
            recv_sem=xrecv.at[j, dx - 1],
            device_id={"tp": lax.rem(x + dx, n_x) * 2 + core},
            device_id_type=MESH,
        )

    def pass_on(j):
        pair_copy(j).wait_recv()
        for dx in range(1, n_x):
            other = lax.rem(x + dx, n_x)
            sbuf[j, dx - 1] = (pbuf[j, core, other].astype(F32) + dbuf[j, other].astype(F32)).astype(BF16)
            cross_copy(j, dx).start()
        own[j] = pbuf[j, core, x].astype(F32) + dbuf[j, x].astype(F32)

    for j in range(chunks):
        cols = slice(j * width, (j + 1) * width)
        part = proj[:, cols] + jnp.dot(attn[:, heads_width:], gw[:, cols], preferred_element_type=F32)
        for b in range(n_tp):
            pbuf[j, b % 2, b // 2] = part[b * out_rows : (b + 1) * out_rows].astype(BF16)
        pair_copy(j).start()
        if j >= 1:
            pass_on(j - 1)
    pass_on(chunks - 1)
    for j in range(chunks):
        value = own[j]
        for dx in range(1, n_x):
            cross_copy(j, dx).wait_recv()
            value = value + rbuf[j, dx - 1].astype(F32)
        out_ref[:, j * width : (j + 1) * width] = value.astype(BF16)

    for j in range(chunks):
        pair_copy(j).wait_send()
        for dx in range(1, n_x):
            cross_copy(j, dx).wait_send()

    @pl.when(has_right)
    def _():
        halo_copy(0).wait_send()

    @pl.when(has_left)
    def _():
        halo_copy(1).wait_send()

    def drain(source, carry):
        for g in range(kvh):
            for part in range(2):
                @pl.when(has_right & (source <= me))
                def _():
                    block_copy(source, g, part, 0).wait_send()

                @pl.when(has_left & (source >= me))
                def _():
                    block_copy(source, g, part, 1).wait_send()

        return carry

    lax.fori_loop(0, n, drain, 0)


def solution(mesh):
    n, n_tp = mesh.shape["sp"], mesh.shape["tp"]

    def per_device(wq, wk, wv, gq, gk, gv, sink, qgain, kgain, ww, gw):
        rows = wq.shape[0]
        kvh = wk.shape[1] // HEAD
        group = wq.shape[1] // wk.shape[1]
        model = ww.shape[1]
        chunks = 8
        width = model // chunks
        n_x = n_tp // 2
        out_rows = rows // n_tp
        heads_width = kvh * group * HEAD
        span = group * rows
        any_spec = pl.BlockSpec(memory_space=pl.ANY)
        vmem = pl.BlockSpec(memory_space=pltpu.VMEM)
        cross = max(n_x - 1, 1)
        return pl.pallas_call(
            functools.partial(kernel, n, n_tp, rows, kvh, group, chunks),
            out_shape=pltpu.VMEM((out_rows, model), BF16),
            in_specs=[any_spec] * 11,
            out_specs=vmem,
            scratch_shapes=[
                pltpu.SMEM(sink.shape, F32),
                pltpu.VMEM((1, HEAD), F32),
                pltpu.VMEM((1, HEAD), F32),
                pltpu.VMEM((kvh, span, HEAD), BF16),
                pltpu.VMEM((kvh, 2, rows + 2 * WINDOW, HEAD), BF16),
                pltpu.VMEM((kvh, span, HEAD), BF16),
                pltpu.VMEM((kvh, rows, HEAD), BF16),
                pltpu.VMEM((kvh, span, HEAD), BF16),
                pltpu.VMEM((n, kvh, 2, rows, HEAD), BF16),
                pltpu.VMEM(ww.shape, BF16),
                pltpu.VMEM(gw.shape, BF16),
                pltpu.VMEM((rows, HEAD), F32),
                pltpu.VMEM((rows, HEAD), F32),
                pltpu.VMEM((kvh, 1, span), F32),
                pltpu.VMEM((kvh, 1, span), F32),
                pltpu.VMEM((kvh, HEAD, span), F32),
                pltpu.VMEM((rows, 2 * heads_width), BF16),
                pltpu.VMEM((rows, model), F32),
                pltpu.VMEM((chunks, 2, n_x, out_rows, width), BF16),
                pltpu.VMEM((chunks, n_x, out_rows, width), BF16),
                pltpu.VMEM((chunks, cross, out_rows, width), BF16),
                pltpu.VMEM((chunks, cross, out_rows, width), BF16),
                pltpu.VMEM((chunks, out_rows, width), F32),
                pltpu.SemaphoreType.DMA((4 * kvh + 2 * kvh * group + 5,)),
                pltpu.SemaphoreType.DMA((2, n, kvh, 2)),
                pltpu.SemaphoreType.DMA((n, kvh, 2)),
                pltpu.SemaphoreType.DMA((2,)),
                pltpu.SemaphoreType.DMA((2,)),
                pltpu.SemaphoreType.DMA((chunks,)),
                pltpu.SemaphoreType.DMA((chunks,)),
                pltpu.SemaphoreType.DMA((chunks, cross)),
                pltpu.SemaphoreType.DMA((chunks, cross)),
            ],
            compiler_params=pltpu.CompilerParams(
                collective_id=0, has_side_effects=True, vmem_limit_bytes=60 * 1024 * 1024
            ),
            name="hybrid",
        )(wq, wk, wv, gq, gk, gv, sink, qgain.reshape(1, HEAD), kgain.reshape(1, HEAD), ww, gw)

    return jax.shard_map(
        per_device,
        mesh=mesh,
        in_specs=(P(("grp", "sp"), "tp"),) * 6 + (P("tp"), P(), P(), P("tp", None), P("tp", None)),
        out_specs=P(("grp", "sp", "tp"), None),
        check_vma=False,
    )
```

```python
import functools
import math

import jax
import jax.numpy as jnp
from jax import lax
from jax.experimental import pallas as pl
from jax.experimental.pallas import tpu as pltpu
from jax.sharding import PartitionSpec as P

HEAD = 128
QH_A = 16
WINDOW = 128
GRID_W = 64
THETA = 10000.0
NEGATIVE = -1e30
EPSILON = 1e-06
LAG = 1
MESH = pl.DeviceIdType.MESH
F32 = jnp.float32
BF16 = jnp.bfloat16


def dot_nt(a, b):
    return lax.dot_general(a, b, (((1,), (1,)), ((), ())), preferred_element_type=F32)


def dot_tn(a, b):
    return lax.dot_general(a, b, (((0,), (0,)), ((), ())), preferred_element_type=F32)


def kernel(
    n, n_tp, rows, kvh, group, chunks, detours,
    wq_hbm, wk_hbm, wv_hbm, gq_hbm, gk_hbm, gv_hbm, sink_hbm, qgain_hbm, kgain_hbm, ww_hbm, gw_hbm,
    out_ref,
    sink_ref, qgain_ref, kgain_ref, qw, wkv, qraw, kraw, qg, kvbuf, ww, gw, cosine, sine, top, total, acc, attn, proj, pbuf, dbuf, sbuf, rbuf, own, detour,
    lsem, gsend, grecv, hsend, hrecv, dsend, drecv, xsend, xrecv, rsend, rrecv,
):
    me = lax.axis_index("sp")
    t = lax.axis_index("tp")
    core = lax.rem(t, 2)
    x = t // 2
    n_x = n_tp // 2
    partner = x * 2 + 1 - core
    out_rows = rows // n_tp
    width = ww.shape[1] // chunks
    span = group * rows
    has_left = me > 0
    has_right = me < n - 1
    at_end = jnp.logical_not(has_left & has_right)
    beside_end = (me == 1) | (me == n - 2)
    inner = jnp.where(me == 0, 1, n - 2)
    outer = jnp.where(me == 1, 0, n - 1)

    barrier = pltpu.get_barrier_semaphore()

    def greet(device):
        pl.semaphore_signal(barrier, inc=1, device_id=device, device_id_type=MESH)

    @pl.when(has_left)
    def _():
        greet({"sp": me - 1})

    @pl.when(has_right)
    def _():
        greet({"sp": me + 1})

    greet({"tp": partner})
    for dx in range(1, n_x):
        greet({"tp": lax.rem(x + dx, n_x) * 2 + core})
    if detours:
        across = lax.rem(x + 1, n_x) * 2 + core

        @pl.when(at_end)
        def _():
            greet({"sp": inner, "tp": across})

        @pl.when(beside_end)
        def _():
            greet({"sp": outer, "tp": across})

    loads = []

    def load(src, dst):
        copy = pltpu.make_async_copy(src, dst, lsem.at[len(loads)])
        copy.start()
        loads.append(copy)
        return copy

    def head_cols(h):
        return slice(h * HEAD, (h + 1) * HEAD)

    v_loads = [load(gv_hbm.at[:, head_cols(g)], kvbuf.at[me, g, 1]) for g in range(kvh)]
    k_loads = [load(gk_hbm.at[:, head_cols(g)], kraw.at[g]) for g in range(kvh)]
    kgain_load = load(kgain_hbm, kgain_ref)
    qgain_load = load(qgain_hbm, qgain_ref)
    sink_load = load(sink_hbm, sink_ref)
    w_loads = []
    for g in range(kvh):
        w_loads.append(load(wk_hbm.at[:, head_cols(g)], wkv.at[g, 0, WINDOW : WINDOW + rows]))
        w_loads.append(load(wv_hbm.at[:, head_cols(g)], wkv.at[g, 1, WINDOW : WINDOW + rows]))
    q_loads = []
    for g in range(kvh):
        for u in range(group):
            q_loads.append(load(gq_hbm.at[:, head_cols(g * group + u)], qraw.at[g, u * rows : (u + 1) * rows]))
    wq_loads = []
    for g in range(kvh):
        for u in range(group):
            wq_loads.append(load(wq_hbm.at[:, head_cols(g * group + u)], qw.at[g, u * rows : (u + 1) * rows]))
    ww_load = load(ww_hbm, ww)
    gw_load = load(gw_hbm, gw)

    section = HEAD // 2
    half = section // 2

    def angles(row_place, column_place, shape):
        lane = lax.broadcasted_iota(jnp.int32, shape, 1)
        frequency = jnp.exp(jnp.bitwise_and(lane, half - 1).astype(F32) * (-2.0 * math.log(THETA) / section))
        return jnp.where(lane < section, row_place, column_place).astype(F32) * frequency

    def signed_sine(angle):
        low = jnp.bitwise_and(lax.broadcasted_iota(jnp.int32, angle.shape, 1), section - 1) < half
        return jnp.where(low, -jnp.sin(angle), jnp.sin(angle))

    def make_tables():
        if rows % GRID_W:
            place = me * rows + lax.broadcasted_iota(jnp.int32, (rows, HEAD), 0)
            angle = angles(place // GRID_W, lax.rem(place, GRID_W), (rows, HEAD))
            cosine[...] = jnp.cos(angle)
            sine[...] = signed_sine(angle)
            return
        lines = rows // GRID_W
        shape = (-(-lines // 8) * 8, HEAD)
        line = me * lines + lax.broadcasted_iota(jnp.int32, shape, 0)
        row_angle = angles(line, line, shape)
        column = lax.broadcasted_iota(jnp.int32, (GRID_W, HEAD), 0)
        column_angle = angles(column, column, (GRID_W, HEAD))
        by_row = lax.broadcasted_iota(jnp.int32, (GRID_W, HEAD), 1) < section
        for table, of in ((cosine, jnp.cos), (sine, signed_sine)):
            per_row, per_column = of(row_angle), of(column_angle)
            for r in range(lines):
                table[r * GRID_W : (r + 1) * GRID_W] = jnp.where(by_row, per_row[r : r + 1], per_column)

    def turn(values, gain):
        v = values.astype(F32)
        v = v * lax.rsqrt(jnp.mean(v * v, axis=1, keepdims=True) + EPSILON) * gain
        first = lax.broadcasted_iota(jnp.int32, v.shape, 1)
        other = jnp.where(
            jnp.bitwise_and(first, section - 1) < half,
            pltpu.roll(v, HEAD - half, 1),
            pltpu.roll(v, half, 1),
        )
        return (v * cosine[...] + other * sine[...]).astype(BF16)

    def block_copy(source, g, part, direction):
        return pltpu.make_async_remote_copy(
            src_ref=kvbuf.at[source, g, part],
            dst_ref=kvbuf.at[source, g, part],
            send_sem=gsend.at[direction, source, g, part],
            recv_sem=grecv.at[source, g, part],
            device_id={"sp": me + 1 if direction == 0 else me - 1},
            device_id_type=MESH,
        )

    def spread(g, part):
        @pl.when(has_right)
        def _():
            block_copy(me, g, part, 0).start()

        @pl.when(has_left)
        def _():
            block_copy(me, g, part, 1).start()

    def halo_copy(direction):
        source = rows if direction == 0 else WINDOW
        target = 0 if direction == 0 else WINDOW + rows
        return pltpu.make_async_remote_copy(
            src_ref=wkv.at[:, :, source : source + WINDOW],
            dst_ref=wkv.at[:, :, target : target + WINDOW],
            send_sem=hsend.at[direction],
            recv_sem=hrecv.at[direction],
            device_id={"sp": me + 1 if direction == 0 else me - 1},
            device_id_type=MESH,
        )

    for copy in v_loads:
        copy.wait()
    greeted = has_left.astype(jnp.int32) + has_right.astype(jnp.int32) + n_x
    if detours:
        greeted = greeted + at_end.astype(jnp.int32) + beside_end.astype(jnp.int32)
    pl.semaphore_wait(barrier, greeted)
    for g in range(kvh):
        spread(g, 1)

    make_tables()
    kgain_load.wait()
    for g in range(kvh):
        k_loads[g].wait()
        kvbuf[me, g, 0] = turn(kraw[g], kgain_ref[...])
        spread(g, 0)

    for copy in w_loads:
        copy.wait()

    @pl.when(has_right)
    def _():
        halo_copy(0).start()

    @pl.when(has_left)
    def _():
        halo_copy(1).start()

    @pl.when(jnp.logical_not(has_left))
    def _():
        wkv[:, :, 0:WINDOW] = jnp.zeros((kvh, 2, WINDOW, HEAD), BF16)

    @pl.when(jnp.logical_not(has_right))
    def _():
        wkv[:, :, WINDOW + rows :] = jnp.zeros((kvh, 2, WINDOW, HEAD), BF16)

    qgain_load.wait()
    for copy in q_loads:
        copy.wait()
    for g in range(kvh):
        for u in range(group):
            part = slice(u * rows, (u + 1) * rows)
            qg[g, part] = turn(qraw[g, part], qgain_ref[...])

    scale = HEAD ** (-0.5)

    def absorb(source, g, first=False):
        scores = dot_nt(kvbuf[source, g, 0], qg[g]) * scale
        block_top = jnp.max(scores, axis=0, keepdims=True)
        if first:
            raised = jnp.exp(scores - block_top)
            top[g] = block_top
            total[g] = jnp.sum(raised, axis=0, keepdims=True)
            acc[g] = dot_tn(kvbuf[source, g, 1], raised.astype(BF16))
        else:
            before = top[g]
            new_top = jnp.maximum(before, block_top)
            fading = jnp.exp(before - new_top)
            raised = jnp.exp(scores - new_top)
            top[g] = new_top
            total[g] = total[g] * fading + jnp.sum(raised, axis=0, keepdims=True)
            acc[g] = acc[g] * fading + dot_tn(kvbuf[source, g, 1], raised.astype(BF16))

    for g in range(kvh):
        absorb(me, g, True)

    def relay(d):
        for part in (1, 0):
            for g in range(kvh):
                @pl.when(me - d >= 0)
                def _():
                    block_copy(me - d, g, part, 0).wait_recv()

                    @pl.when(has_right)
                    def _():
                        block_copy(me - d, g, part, 0).start()

                @pl.when(me + d < n)
                def _():
                    block_copy(me + d, g, part, 1).wait_recv()

                    @pl.when(has_left)
                    def _():
                        block_copy(me + d, g, part, 1).start()

                if part == 0:
                    @pl.when(me - d >= 0)
                    def _():
                        absorb(me - d, g)

                    @pl.when(me + d < n)
                    def _():
                        absorb(me + d, g)

    def put_heads(base, g, value):
        turned = jnp.transpose(value).astype(BF16)
        for u in range(group):
            attn[:, base + (g * group + u) * HEAD : base + (g * group + u + 1) * HEAD] = turned[u * rows : (u + 1) * rows]

    heads_width = kvh * group * HEAD

    def windowed():
        sink_load.wait()
        for copy in wq_loads:
            copy.wait()

        @pl.when(has_left)
        def _():
            halo_copy(0).wait_recv()

        @pl.when(has_right)
        def _():
            halo_copy(1).wait_recv()

        padded = rows + 2 * WINDOW
        key_at = lax.broadcasted_iota(jnp.int32, (padded, span), 0) - WINDOW
        column = lax.broadcasted_iota(jnp.int32, (padded, span), 1)
        distance = jnp.abs(key_at - lax.rem(column, rows))
        key_place = me * rows + key_at
        inside = (distance <= WINDOW) & (key_place >= 0) & (key_place < n * rows)
        far = distance.astype(F32)
        member = lax.broadcasted_iota(jnp.int32, (1, span), 1) // rows
        for g in range(kvh):
            head = (t * (kvh * group) + g * group + 1 + member).astype(F32)
            slope = jnp.exp2(head * (-8.0 / QH_A))
            sink = jnp.zeros((1, span), F32)
            for u in range(group):
                sink = jnp.where(member == u, sink_ref[g * group + u], sink)
            scores = dot_nt(wkv[g, 0], qw[g]) * scale
            scores = jnp.where(inside, scores - slope * far, NEGATIVE)
            highest = jnp.maximum(jnp.max(scores, axis=0, keepdims=True), sink)
            raised = jnp.exp(scores - highest)
            bottom = jnp.sum(raised, axis=0, keepdims=True) + jnp.exp(sink - highest)
            weights = (raised * (1.0 / bottom)).astype(BF16)
            put_heads(0, g, dot_tn(wkv[g, 1], weights))
        ww_load.wait()
        for j in range(chunks):
            cols = slice(j * width, (j + 1) * width)
            proj[:, cols] = jnp.dot(attn[:, :heads_width], ww[:, cols], preferred_element_type=F32)

    if n > 1:
        relay(1)
    windowed()
    if n <= 4:
        for d in range(2, n):
            relay(d)
    else:
        def relay_step(d, carry):
            relay(d)
            return carry

        lax.fori_loop(2, n, relay_step, 0)

    for g in range(kvh):
        put_heads(heads_width, g, acc[g] * (1.0 / total[g]))
    gw_load.wait()

    def pair_copy(j):
        return pltpu.make_async_remote_copy(
            src_ref=pbuf.at[j, 1 - core],
            dst_ref=dbuf.at[j],
            send_sem=dsend.at[j],
            recv_sem=drecv.at[j],
            device_id={"tp": partner},
            device_id_type=MESH,
        )

    def cross_copy(j, dx):
        return pltpu.make_async_remote_copy(
            src_ref=sbuf.at[j, dx - 1],
            dst_ref=rbuf.at[j, dx - 1],
            send_sem=xsend.at[j, dx - 1],
            recv_sem=xrecv.at[j, dx - 1],
            device_id={"tp": lax.rem(x + dx, n_x) * 2 + core},
            device_id_type=MESH,
        )

    def detour_copy(j):
        return pltpu.make_async_remote_copy(
            src_ref=sbuf.at[j, 0],
            dst_ref=detour.at[detours.index(j)],
            send_sem=xsend.at[j, 0],
            recv_sem=rrecv.at[detours.index(j)],
            device_id={"sp": inner, "tp": across},
            device_id_type=MESH,
        )

    def detour_end_copy(j):
        return pltpu.make_async_remote_copy(
            src_ref=detour.at[detours.index(j)],
            dst_ref=rbuf.at[j, 0],
            send_sem=rsend.at[detours.index(j)],
            recv_sem=xrecv.at[j, 0],
            device_id={"sp": outer},
            device_id_type=MESH,
        )

    def pass_on(j):
        pair_copy(j).wait_recv()
        for dx in range(1, n_x):
            other = lax.rem(x + dx, n_x)
            sbuf[j, dx - 1] = (pbuf[j, core, other].astype(F32) + dbuf[j, other].astype(F32)).astype(BF16)
            if j in detours:
                @pl.when(at_end)
                def _():
                    detour_copy(j).start()

                @pl.when(jnp.logical_not(at_end))
                def _():
                    cross_copy(j, dx).start()
            else:
                cross_copy(j, dx).start()
        own[j] = pbuf[j, core, x].astype(F32) + dbuf[j, x].astype(F32)

    for j in range(chunks):
        cols = slice(j * width, (j + 1) * width)
        part = proj[:, cols] + jnp.dot(attn[:, heads_width:], gw[:, cols], preferred_element_type=F32)
        for b in range(n_tp):
            pbuf[j, b % 2, b // 2] = part[b * out_rows : (b + 1) * out_rows].astype(BF16)
        pair_copy(j).start()
        if j >= LAG:
            pass_on(j - LAG)
    for j in range(chunks - LAG, chunks):
        pass_on(j)
    for j in detours:
        @pl.when(beside_end)
        def _():
            detour_copy(j).wait_recv()
            detour_end_copy(j).start()

    for j in range(chunks):
        value = own[j]
        for dx in range(1, n_x):
            cross_copy(j, dx).wait_recv()
            value = value + rbuf[j, dx - 1].astype(F32)
        out_ref[:, j * width : (j + 1) * width] = value.astype(BF16)

    for j in range(chunks):
        pair_copy(j).wait_send()
        for dx in range(1, n_x):
            cross_copy(j, dx).wait_send()
    for j in detours:
        @pl.when(beside_end)
        def _():
            detour_end_copy(j).wait_send()

    @pl.when(has_right)
    def _():
        halo_copy(0).wait_send()

    @pl.when(has_left)
    def _():
        halo_copy(1).wait_send()

    def drain(source, carry):
        for g in range(kvh):
            for part in range(2):
                @pl.when(has_right & (source <= me))
                def _():
                    block_copy(source, g, part, 0).wait_send()

                @pl.when(has_left & (source >= me))
                def _():
                    block_copy(source, g, part, 1).wait_send()

        return carry

    lax.fori_loop(0, n, drain, 0)


def solution(mesh):
    n, n_tp = mesh.shape["sp"], mesh.shape["tp"]

    def per_device(wq, wk, wv, gq, gk, gv, sink, qgain, kgain, ww, gw):
        rows = wq.shape[0]
        kvh = wk.shape[1] // HEAD
        group = wq.shape[1] // wk.shape[1]
        model = ww.shape[1]
        chunks = 8
        width = model // chunks
        n_x = n_tp // 2
        out_rows = rows // n_tp
        heads_width = kvh * group * HEAD
        span = group * rows
        any_spec = pl.BlockSpec(memory_space=pl.ANY)
        vmem = pl.BlockSpec(memory_space=pltpu.VMEM)
        cross = max(n_x - 1, 1)
        detours = (1, 3) if n >= 4 and n_x == 2 else ()
        return pl.pallas_call(
            functools.partial(kernel, n, n_tp, rows, kvh, group, chunks, detours),
            out_shape=pltpu.VMEM((out_rows, model), BF16),
            in_specs=[any_spec] * 11,
            out_specs=vmem,
            scratch_shapes=[
                pltpu.SMEM(sink.shape, F32),
                pltpu.VMEM((1, HEAD), F32),
                pltpu.VMEM((1, HEAD), F32),
                pltpu.VMEM((kvh, span, HEAD), BF16),
                pltpu.VMEM((kvh, 2, rows + 2 * WINDOW, HEAD), BF16),
                pltpu.VMEM((kvh, span, HEAD), BF16),
                pltpu.VMEM((kvh, rows, HEAD), BF16),
                pltpu.VMEM((kvh, span, HEAD), BF16),
                pltpu.VMEM((n, kvh, 2, rows, HEAD), BF16),
                pltpu.VMEM(ww.shape, BF16),
                pltpu.VMEM(gw.shape, BF16),
                pltpu.VMEM((rows, HEAD), F32),
                pltpu.VMEM((rows, HEAD), F32),
                pltpu.VMEM((kvh, 1, span), F32),
                pltpu.VMEM((kvh, 1, span), F32),
                pltpu.VMEM((kvh, HEAD, span), F32),
                pltpu.VMEM((rows, 2 * heads_width), BF16),
                pltpu.VMEM((rows, model), F32),
                pltpu.VMEM((chunks, 2, n_x, out_rows, width), BF16),
                pltpu.VMEM((chunks, n_x, out_rows, width), BF16),
                pltpu.VMEM((chunks, cross, out_rows, width), BF16),
                pltpu.VMEM((chunks, cross, out_rows, width), BF16),
                pltpu.VMEM((chunks, out_rows, width), F32),
                pltpu.VMEM((max(len(detours), 1), out_rows, width), BF16),
                pltpu.SemaphoreType.DMA((4 * kvh + 2 * kvh * group + 5,)),
                pltpu.SemaphoreType.DMA((2, n, kvh, 2)),
                pltpu.SemaphoreType.DMA((n, kvh, 2)),
                pltpu.SemaphoreType.DMA((2,)),
                pltpu.SemaphoreType.DMA((2,)),
                pltpu.SemaphoreType.DMA((chunks,)),
                pltpu.SemaphoreType.DMA((chunks,)),
                pltpu.SemaphoreType.DMA((chunks, cross)),
                pltpu.SemaphoreType.DMA((chunks, cross)),
                pltpu.SemaphoreType.DMA((max(len(detours), 1),)),
                pltpu.SemaphoreType.DMA((max(len(detours), 1),)),
            ],
            compiler_params=pltpu.CompilerParams(
                collective_id=0, has_side_effects=True, vmem_limit_bytes=60 * 1024 * 1024
            ),
            name="hybrid",
        )(wq, wk, wv, gq, gk, gv, sink, qgain.reshape(1, HEAD), kgain.reshape(1, HEAD), ww, gw)

    return jax.shard_map(
        per_device,
        mesh=mesh,
        in_specs=(P(("grp", "sp"), "tp"),) * 6 + (P("tp"), P(), P(), P("tp", None), P("tp", None)),
        out_specs=P(("grp", "sp", "tp"), None),
        check_vma=False,
    )
```

```python
import functools
import math

import jax
import jax.numpy as jnp
from jax import lax
from jax.experimental import pallas as pl
from jax.experimental.pallas import tpu as pltpu
from jax.sharding import PartitionSpec as P

HEAD = 128
QH_A = 16
WINDOW = 128
GRID_W = 64
THETA = 10000.0
AWAY = 1e30
EPSILON = 1e-06
DIRECT = 128
LEND = True
MESH = pl.DeviceIdType.MESH
F32 = jnp.float32
BF16 = jnp.bfloat16


def dot_nt(a, b):
    return lax.dot_general(a, b, (((1,), (1,)), ((), ())), preferred_element_type=F32)


def dot_tn(a, b):
    return lax.dot_general(a, b, (((0,), (0,)), ((), ())), preferred_element_type=F32)


def kernel(
    n, n_tp, rows, kvh, group, cuts, direct, detours, lend,
    wq_hbm, wk_hbm, wv_hbm, gq_hbm, gk_hbm, gv_hbm, sink_hbm, qgain_hbm, kgain_hbm, ww_hbm, gw_hbm,
    out_ref,
    sink_ref, qgain_ref, kgain_ref, qw, wkv, qraw, kraw, qg, kvbuf, ww, gw, cosine, sine, top, total, acc, attn, proj, pbuf, dbuf, sbuf, rbuf, own, detour, lent, lent_sums, xbuf, far,
    lsem, gsend, grecv, hsend, hrecv, dsend, drecv, xsend, xrecv, rsend, rrecv, lsend, lrecv, usend, urecv,
):
    me = lax.axis_index("sp")
    t = lax.axis_index("tp")
    core = lax.rem(t, 2)
    x = t // 2
    n_x = n_tp // 2
    partner = x * 2 + 1 - core
    out_rows = rows // n_tp
    chunks = len(cuts)
    span = group * rows
    spans = [slice(begin, end) for begin, end in cuts]
    sizes = [slice(0, end - begin) for begin, end in cuts]
    has_left = me > 0
    has_right = me < n - 1
    at_end = jnp.logical_not(has_left & has_right)
    beside_end = (me == 1) | (me == n - 2)
    inner = jnp.where(me == 0, 1, n - 2)
    outer = jnp.where(me == 1, 0, n - 1)
    last = kvh - 1
    near = jnp.where(me >= n // 2, 0, 1)

    barrier = pltpu.get_barrier_semaphore()

    def greet(device):
        pl.semaphore_signal(barrier, inc=1, device_id=device, device_id_type=MESH)

    @pl.when(has_left)
    def _():
        greet({"sp": me - 1})

    @pl.when(has_right)
    def _():
        greet({"sp": me + 1})

    greet({"tp": partner})
    for dx in range(1, n_x):
        greet({"tp": lax.rem(x + dx, n_x) * 2 + core})
    if direct:
        greet({"tp": lax.rem(x + 1, n_x) * 2 + 1 - core})
    if detours:
        across = lax.rem(x + 1, n_x) * 2 + core

        @pl.when(at_end)
        def _():
            greet({"sp": inner, "tp": across})

        @pl.when(beside_end)
        def _():
            greet({"sp": outer, "tp": across})

    loads = []

    def load(src, dst):
        copy = pltpu.make_async_copy(src, dst, lsem.at[len(loads)])
        copy.start()
        loads.append(copy)
        return copy

    def head_cols(h):
        return slice(h * HEAD, (h + 1) * HEAD)

    v_loads = [load(gv_hbm.at[:, head_cols(g)], kvbuf.at[me, g, 1]) for g in range(kvh)]
    k_loads = [load(gk_hbm.at[:, head_cols(g)], kraw.at[g]) for g in range(kvh)]
    kgain_load = load(kgain_hbm, kgain_ref)
    qgain_load = load(qgain_hbm, qgain_ref)
    sink_load = load(sink_hbm, sink_ref)
    w_loads = []
    for g in range(kvh):
        w_loads.append(load(wk_hbm.at[:, head_cols(g)], wkv.at[g, 0, WINDOW : WINDOW + rows]))
        w_loads.append(load(wv_hbm.at[:, head_cols(g)], wkv.at[g, 1, WINDOW : WINDOW + rows]))
    q_loads = []
    for g in range(kvh):
        for u in range(group):
            q_loads.append(load(gq_hbm.at[:, head_cols(g * group + u)], qraw.at[g, u * rows : (u + 1) * rows]))
    wq_loads = []
    for g in range(kvh):
        for u in range(group):
            wq_loads.append(load(wq_hbm.at[:, head_cols(g * group + u)], qw.at[g, u * rows : (u + 1) * rows]))
    ww_load = load(ww_hbm, ww)
    gw_load = load(gw_hbm, gw)

    section = HEAD // 2
    half = section // 2

    def angles(row_place, column_place, shape):
        lane = lax.broadcasted_iota(jnp.int32, shape, 1)
        frequency = jnp.exp(jnp.bitwise_and(lane, half - 1).astype(F32) * (-2.0 * math.log(THETA) / section))
        return jnp.where(lane < section, row_place, column_place).astype(F32) * frequency

    def signed_sine(angle):
        low = jnp.bitwise_and(lax.broadcasted_iota(jnp.int32, angle.shape, 1), section - 1) < half
        return jnp.where(low, -jnp.sin(angle), jnp.sin(angle))

    def make_tables():
        if rows % GRID_W:
            place = me * rows + lax.broadcasted_iota(jnp.int32, (rows, HEAD), 0)
            angle = angles(place // GRID_W, lax.rem(place, GRID_W), (rows, HEAD))
            cosine[...] = jnp.cos(angle)
            sine[...] = signed_sine(angle)
            return
        lines = rows // GRID_W
        shape = (-(-lines // 8) * 8, HEAD)
        line = me * lines + lax.broadcasted_iota(jnp.int32, shape, 0)
        row_angle = angles(line, line, shape)
        column = lax.broadcasted_iota(jnp.int32, (GRID_W, HEAD), 0)
        column_angle = angles(column, column, (GRID_W, HEAD))
        by_row = lax.broadcasted_iota(jnp.int32, (GRID_W, HEAD), 1) < section
        for table, of in ((cosine, jnp.cos), (sine, signed_sine)):
            per_row, per_column = of(row_angle), of(column_angle)
            for r in range(lines):
                table[r * GRID_W : (r + 1) * GRID_W] = jnp.where(by_row, per_row[r : r + 1], per_column)

    def turn(values, gain):
        v = values.astype(F32)
        v = v * lax.rsqrt(jnp.mean(v * v, axis=1, keepdims=True) + EPSILON) * gain
        first = lax.broadcasted_iota(jnp.int32, v.shape, 1)
        other = jnp.where(
            jnp.bitwise_and(first, section - 1) < half,
            pltpu.roll(v, HEAD - half, 1),
            pltpu.roll(v, half, 1),
        )
        return (v * cosine[...] + other * sine[...]).astype(BF16)

    def block_copy(source, g, part, way):
        return pltpu.make_async_remote_copy(
            src_ref=kvbuf.at[source, g, part],
            dst_ref=kvbuf.at[source, g, part],
            send_sem=gsend.at[way, source, g, part],
            recv_sem=grecv.at[source, g, part],
            device_id={"sp": me + 1 - 2 * way},
            device_id_type=MESH,
        )

    def spread(g, part):
        kept = lend and g == last

        @pl.when((me < n - 2) if kept else has_right)
        def _():
            block_copy(me, g, part, 0).start()

        @pl.when((me > 1) if kept else has_left)
        def _():
            block_copy(me, g, part, 1).start()

    def lend_queries():
        return pltpu.make_async_remote_copy(
            src_ref=qg.at[last],
            dst_ref=qg.at[kvh],
            send_sem=lsend.at[0],
            recv_sem=lrecv.at[0],
            device_id={"sp": inner},
            device_id_type=MESH,
        )

    def return_lent():
        return [
            pltpu.make_async_remote_copy(
                src_ref=ref,
                dst_ref=ref,
                send_sem=lsend.at[1 + i],
                recv_sem=lrecv.at[1 + i],
                device_id={"sp": outer},
                device_id_type=MESH,
            )
            for i, ref in enumerate((lent, lent_sums))
        ]

    def halo_copy(direction):
        source = rows if direction == 0 else WINDOW
        target = 0 if direction == 0 else WINDOW + rows
        return pltpu.make_async_remote_copy(
            src_ref=wkv.at[:, :, source : source + WINDOW],
            dst_ref=wkv.at[:, :, target : target + WINDOW],
            send_sem=hsend.at[direction],
            recv_sem=hrecv.at[direction],
            device_id={"sp": me + 1 if direction == 0 else me - 1},
            device_id_type=MESH,
        )

    def start_halos():
        @pl.when(has_right)
        def _():
            halo_copy(0).start()

        @pl.when(has_left)
        def _():
            halo_copy(1).start()

    def turn_queries(g):
        for u in range(group):
            q_loads[g * group + u].wait()
        for u in range(group):
            part = slice(u * rows, (u + 1) * rows)
            qg[g, part] = turn(qraw[g, part], qgain_ref[...])

    make_tables()
    for copy in v_loads:
        copy.wait()
    greeted = has_left.astype(jnp.int32) + has_right.astype(jnp.int32) + n_x + (1 if direct else 0)
    if detours:
        greeted = greeted + at_end.astype(jnp.int32) + beside_end.astype(jnp.int32)
    pl.semaphore_wait(barrier, greeted)
    spread(0, 1)
    if lend:
        qgain_load.wait()
        turn_queries(last)

        @pl.when(at_end)
        def _():
            lend_queries().start()

    for g in range(1, kvh):
        spread(g, 1)
    for copy in w_loads:
        copy.wait()
    if lend:
        @pl.when(at_end)
        def _():
            start_halos()

    kgain_load.wait()
    for g in range(kvh):
        k_loads[g].wait()
        kvbuf[me, g, 0] = turn(kraw[g], kgain_ref[...])
        spread(g, 0)
    if lend:
        @pl.when(jnp.logical_not(at_end))
        def _():
            start_halos()
    else:
        start_halos()

    @pl.when(jnp.logical_not(has_left))
    def _():
        wkv[:, :, 0:WINDOW] = jnp.zeros((kvh, 2, WINDOW, HEAD), BF16)

    @pl.when(jnp.logical_not(has_right))
    def _():
        wkv[:, :, WINDOW + rows :] = jnp.zeros((kvh, 2, WINDOW, HEAD), BF16)

    if not lend:
        qgain_load.wait()
    for g in range(kvh - 1 if lend else kvh):
        turn_queries(g)

    scale = HEAD ** (-0.5)

    def absorb(source, g, first=False, slot=None):
        slot = g if slot is None else slot
        scores = dot_nt(kvbuf[source, g, 0], qg[slot]) * scale
        block_top = jnp.max(scores, axis=0, keepdims=True)
        if first:
            raised = jnp.exp(scores - block_top)
            top[slot] = block_top
            total[slot] = jnp.sum(raised, axis=0, keepdims=True)
            acc[slot] = dot_tn(kvbuf[source, g, 1], raised.astype(BF16))
        else:
            before = top[slot]
            new_top = jnp.maximum(before, block_top)
            fading = jnp.exp(before - new_top)
            raised = jnp.exp(scores - new_top)
            top[slot] = new_top
            total[slot] = total[slot] * fading + jnp.sum(raised, axis=0, keepdims=True)
            acc[slot] = acc[slot] * fading + dot_tn(kvbuf[source, g, 1], raised.astype(BF16))

    for g in range(kvh):
        absorb(me, g, True)

    def there(d, way, g):
        source = me - (1 - 2 * way) * d
        comes = (source >= 0) & (source < n)
        if lend and g == last and isinstance(d, int) and d <= 2:
            comes = comes & jnp.logical_not(at_end)
        return source, comes

    def piece(d, way, g, part):
        source, comes = there(d, way, g)
        target = me + 1 - 2 * way

        @pl.when(comes)
        def _():
            block_copy(source, g, part, way).wait_recv()
            kept = lend and g == last and isinstance(d, int) and d <= 1
            goes = (target > 0) & (target < n - 1) if kept else (target >= 0) & (target < n)

            @pl.when(goes)
            def _():
                block_copy(source, g, part, way).start()

    def take(d, way, g):
        source, comes = there(d, way, g)

        @pl.when(comes)
        def _():
            absorb(source, g)

    def take_all(d, way):
        if lend and d <= 2:
            source = me - (1 - 2 * way) * d
            inside = (source >= 0) & (source < n)

            @pl.when(inside & jnp.logical_not(at_end))
            def _():
                for g in range(kvh):
                    absorb(source, g)

            @pl.when(inside & at_end)
            def _():
                for g in range(last):
                    absorb(source, g)
        else:
            source, comes = there(d, way, 0)

            @pl.when(comes)
            def _():
                for g in range(kvh):
                    absorb(source, g)

    def relay_near():
        far_way = 1 - near
        for g in range(kvh):
            piece(1, near, g, 1)
        piece(1, far_way, 0, 1)
        for g in range(kvh):
            if lend and g == last:
                @pl.when(beside_end)
                def _():
                    lend_queries().wait_recv()
                    absorb(me, last, True, kvh)

            piece(1, near, g, 0)
        if lend:
            @pl.when(beside_end)
            def _():
                absorb(there(1, near, last)[0], last, False, kvh)
                lent[...] = (acc[kvh] * (1.0 / total[kvh])).astype(BF16)
                lent_sums[0] = top[kvh]
                lent_sums[1] = total[kvh]
                for copy in return_lent():
                    copy.start()

        for g in range(1, kvh):
            piece(1, far_way, g, 1)
        take_all(1, near)

    def relay(d):
        ways = [near, 1 - near] if not isinstance(d, int) or d < n - n // 2 else [near]
        for part in (1, 0):
            for g in range(kvh):
                for way in ways:
                    piece(d, way, g, part)
                if part == 0:
                    for way in ways:
                        take(d, way, g)
                    if n == 4:
                        @pl.when(at_end)
                        def _():
                            finish(g)

    def relay_far_and_second():
        other = 1 - near
        ways = (near, other)[: 2 if n > 4 else 1]

        def second(g, part):
            for way in ways if n > 2 else ():
                piece(2, way, g, part)

        def take_second(g):
            for way in ways if n > 2 else ():
                take(2, way, g)

        window_head(0)
        piece(1, other, 0, 0)
        second(0, 1)
        for g in range(1, kvh):
            window_head(g)
        take(1, other, 0)
        for g in range(1, kvh):
            piece(1, other, g, 0)
            second(g, 1)
            take(1, other, g)
        window_project(0, chunks)
        for g in range(kvh):
            second(g, 0)
            take_second(g)
            if n == 4:
                @pl.when(jnp.logical_not(at_end))
                def _():
                    finish(g)

    def merge_lent():
        for copy in return_lent():
            copy.wait_recv()
        before = top[last]
        new_top = jnp.maximum(before, lent_sums[0])
        fading = jnp.exp(before - new_top)
        share = jnp.exp(lent_sums[0] - new_top) * lent_sums[1]
        top[last] = new_top
        total[last] = total[last] * fading + share
        acc[last] = acc[last] * fading + lent[...].astype(F32) * share

    def put_heads(base, g, value):
        turned = jnp.transpose(value).astype(BF16)
        for u in range(group):
            attn[:, base + (g * group + u) * HEAD : base + (g * group + u + 1) * HEAD] = turned[u * rows : (u + 1) * rows]

    heads_width = kvh * group * HEAD

    def finish(g):
        put_heads(heads_width, g, acc[g] * (1.0 / total[g]))

    def window_inputs():
        sink_load.wait()
        for copy in wq_loads:
            copy.wait()

        @pl.when(has_left)
        def _():
            halo_copy(0).wait_recv()

        @pl.when(has_right)
        def _():
            halo_copy(1).wait_recv()

    padded = rows + 2 * WINDOW

    def make_distances():
        key_at = lax.broadcasted_iota(jnp.int32, (padded, span), 0) - WINDOW
        column = lax.broadcasted_iota(jnp.int32, (1, span), 1)
        distance = jnp.abs(key_at - lax.rem(column, rows))
        key_place = me * rows + lax.broadcasted_iota(jnp.int32, (padded, 1), 0) - WINDOW
        reach = jnp.where((key_place >= 0) & (key_place < n * rows), WINDOW, -1)
        far[...] = jnp.where(distance <= reach, distance.astype(F32), AWAY)

    def window_head(g):
        if g == 0:
            window_inputs()
        member = lax.broadcasted_iota(jnp.int32, (1, span), 1) // rows
        head = (t * (kvh * group) + g * group + 1 + member).astype(F32)
        slope = jnp.exp2(head * (-8.0 / QH_A))
        sink = jnp.zeros((1, span), F32)
        for u in range(group):
            sink = jnp.where(member == u, sink_ref[g * group + u], sink)
        scores = dot_nt(wkv[g, 0], qw[g]) * scale
        scores = scores - slope * far[...]
        highest = jnp.maximum(jnp.max(scores, axis=0, keepdims=True), sink)
        raised = jnp.exp(scores - highest)
        bottom = jnp.sum(raised, axis=0, keepdims=True) + jnp.exp(sink - highest)
        weights = (raised * (1.0 / bottom)).astype(BF16)
        put_heads(0, g, dot_tn(wkv[g, 1], weights))

    def window_project(begin, end):
        if begin == 0:
            ww_load.wait()
        for j in range(begin, end):
            cols = spans[j]
            proj[:, cols] = jnp.dot(attn[:, :heads_width], ww[:, cols], preferred_element_type=F32)

    make_distances()
    if n > 1:
        relay_near()
    if n > 1:
        relay_far_and_second()
    else:
        for g in range(kvh):
            window_head(g)
        window_project(0, chunks)
    if lend:
        @pl.when(at_end)
        def _():
            merge_lent()

    if n <= 4:
        for d in range(3, n):
            relay(d)
    else:
        def relay_step(d, carry):
            relay(d)
            return carry

        lax.fori_loop(3, n, relay_step, 0)

    if n != 4:
        for g in range(kvh):
            finish(g)
    gw_load.wait()

    def pair_copy(j):
        return pltpu.make_async_remote_copy(
            src_ref=pbuf.at[j, 1 - core, :, :, sizes[j]],
            dst_ref=dbuf.at[j, :, :, sizes[j]],
            send_sem=dsend.at[j],
            recv_sem=drecv.at[j],
            device_id={"tp": partner},
            device_id_type=MESH,
        )

    def cross_copy(j, dx):
        return pltpu.make_async_remote_copy(
            src_ref=sbuf.at[j, dx - 1, :, sizes[j]],
            dst_ref=rbuf.at[j, dx - 1, :, sizes[j]],
            send_sem=xsend.at[j, dx - 1],
            recv_sem=xrecv.at[j, dx - 1],
            device_id={"tp": lax.rem(x + dx, n_x) * 2 + core},
            device_id_type=MESH,
        )

    def direct_pair_copy(j):
        return pltpu.make_async_remote_copy(
            src_ref=pbuf.at[j, 1 - core, x, :, sizes[j]],
            dst_ref=dbuf.at[j, x, :, sizes[j]],
            send_sem=dsend.at[j],
            recv_sem=drecv.at[j],
            device_id={"tp": partner},
            device_id_type=MESH,
        )

    def direct_copy(j, flip):
        to = core if flip == 0 else 1 - core
        return pltpu.make_async_remote_copy(
            src_ref=pbuf.at[j, to, lax.rem(x + 1, n_x), :, sizes[j]],
            dst_ref=xbuf.at[j, flip, :, sizes[j]],
            send_sem=usend.at[j, flip],
            recv_sem=urecv.at[j, flip],
            device_id={"tp": lax.rem(x + 1, n_x) * 2 + to},
            device_id_type=MESH,
        )

    def detour_copy(j):
        return pltpu.make_async_remote_copy(
            src_ref=sbuf.at[j, 0],
            dst_ref=detour.at[detours.index(j)],
            send_sem=xsend.at[j, 0],
            recv_sem=rrecv.at[detours.index(j)],
            device_id={"sp": inner, "tp": across},
            device_id_type=MESH,
        )

    def detour_end_copy(j):
        return pltpu.make_async_remote_copy(
            src_ref=detour.at[detours.index(j)],
            dst_ref=rbuf.at[j, 0],
            send_sem=rsend.at[detours.index(j)],
            recv_sem=xrecv.at[j, 0],
            device_id={"sp": outer},
            device_id_type=MESH,
        )

    def pass_on(j):
        pair_copy(j).wait_recv()
        for dx in range(1, n_x):
            other = lax.rem(x + dx, n_x)
            both = pbuf[j, core, other, :, sizes[j]].astype(F32) + dbuf[j, other, :, sizes[j]].astype(F32)
            sbuf[j, dx - 1, :, sizes[j]] = both.astype(BF16)
            if j in detours:
                @pl.when(at_end)
                def _():
                    detour_copy(j).start()

                @pl.when(jnp.logical_not(at_end))
                def _():
                    cross_copy(j, dx).start()
            else:
                cross_copy(j, dx).start()
        own[j, :, sizes[j]] = pbuf[j, core, x, :, sizes[j]].astype(F32) + dbuf[j, x, :, sizes[j]].astype(F32)

    def project(j):
        part = proj[:, spans[j]] + jnp.dot(attn[:, heads_width:], gw[:, spans[j]], preferred_element_type=F32)
        for b in range(n_tp):
            pbuf[j, b % 2, b // 2, :, sizes[j]] = part[b * out_rows : (b + 1) * out_rows].astype(BF16)
        if j < direct:
            direct_pair_copy(j).start()
            for c in range(2):
                direct_copy(j, c).start()
        else:
            pair_copy(j).start()

    for j in range(direct + 1):
        project(j)
    project(direct + 1)
    pass_on(direct)
    for j in range(direct + 2, chunks):
        project(j)
        if j > direct + 2:
            pass_on(j - 2)
    for j in range(chunks - 2, chunks):
        pass_on(j)

    for j in detours:
        @pl.when(beside_end)
        def _():
            detour_copy(j).wait_recv()
            detour_end_copy(j).start()

    for j in range(direct):
        direct_pair_copy(j).wait()
        for c in range(2):
            direct_copy(j, c).wait()
        value = pbuf[j, core, x, :, sizes[j]].astype(F32) + dbuf[j, x, :, sizes[j]].astype(F32)
        for c in range(2):
            value = value + xbuf[j, c, :, sizes[j]].astype(F32)
        out_ref[:, spans[j]] = value.astype(BF16)
    for j in range(direct, chunks):
        value = own[j, :, sizes[j]]
        for dx in range(1, n_x):
            cross_copy(j, dx).wait_recv()
            value = value + rbuf[j, dx - 1, :, sizes[j]].astype(F32)
        out_ref[:, spans[j]] = value.astype(BF16)

    for j in range(direct, chunks):
        pair_copy(j).wait_send()
        for dx in range(1, n_x):
            cross_copy(j, dx).wait_send()
    for j in detours:
        @pl.when(beside_end)
        def _():
            detour_end_copy(j).wait_send()

    @pl.when(has_right)
    def _():
        halo_copy(0).wait_send()

    @pl.when(has_left)
    def _():
        halo_copy(1).wait_send()

    if lend:
        @pl.when(at_end)
        def _():
            lend_queries().wait_send()

        @pl.when(beside_end)
        def _():
            for copy in return_lent():
                copy.wait_send()

    def drain(source, carry):
        for g in range(kvh):
            right = has_right & (source <= me)
            left = has_left & (source >= me)
            if lend and g == last:
                right = right & jnp.logical_not((me == n - 2) & (source >= n - 3))
                left = left & jnp.logical_not((me == 1) & (source <= 2))
            for part in range(2):
                @pl.when(right)
                def _():
                    block_copy(source, g, part, 0).wait_send()

                @pl.when(left)
                def _():
                    block_copy(source, g, part, 1).wait_send()

        return carry

    lax.fori_loop(0, n, drain, 0)


def solution(mesh):
    n, n_tp = mesh.shape["sp"], mesh.shape["tp"]

    def per_device(wq, wk, wv, gq, gk, gv, sink, qgain, kgain, ww, gw):
        rows = wq.shape[0]
        kvh = wk.shape[1] // HEAD
        group = wq.shape[1] // wk.shape[1]
        model = ww.shape[1]
        chunks = 8
        width = model // chunks
        cuts = [(j * width, (j + 1) * width) for j in range(chunks)]
        direct = 0
        n_x = n_tp // 2
        out_rows = rows // n_tp
        heads_width = kvh * group * HEAD
        span = group * rows
        if n_tp == 4 and width > DIRECT:
            direct = 1
            cuts = [(0, DIRECT), (DIRECT, width)] + cuts[1:]
        chunks = len(cuts)
        any_spec = pl.BlockSpec(memory_space=pl.ANY)
        vmem = pl.BlockSpec(memory_space=pltpu.VMEM)
        cross = max(n_x - 1, 1)
        lend = LEND and n >= 4 and kvh >= 2
        detours = (3,) if n >= 4 and n_x == 2 else ()
        return pl.pallas_call(
            functools.partial(kernel, n, n_tp, rows, kvh, group, cuts, direct, detours, lend),
            out_shape=pltpu.VMEM((out_rows, model), BF16),
            in_specs=[any_spec] * 11,
            out_specs=vmem,
            scratch_shapes=[
                pltpu.SMEM(sink.shape, F32),
                pltpu.VMEM((1, HEAD), F32),
                pltpu.VMEM((1, HEAD), F32),
                pltpu.VMEM((kvh, span, HEAD), BF16),
                pltpu.VMEM((kvh, 2, rows + 2 * WINDOW, HEAD), BF16),
                pltpu.VMEM((kvh, span, HEAD), BF16),
                pltpu.VMEM((kvh, rows, HEAD), BF16),
                pltpu.VMEM((kvh + lend, span, HEAD), BF16),
                pltpu.VMEM((n, kvh, 2, rows, HEAD), BF16),
                pltpu.VMEM(ww.shape, BF16),
                pltpu.VMEM(gw.shape, BF16),
                pltpu.VMEM((rows, HEAD), F32),
                pltpu.VMEM((rows, HEAD), F32),
                pltpu.VMEM((kvh + lend, 1, span), F32),
                pltpu.VMEM((kvh + lend, 1, span), F32),
                pltpu.VMEM((kvh + lend, HEAD, span), F32),
                pltpu.VMEM((rows, 2 * heads_width), BF16),
                pltpu.VMEM((rows, model), F32),
                pltpu.VMEM((chunks, 2, n_x, out_rows, width), BF16),
                pltpu.VMEM((chunks, n_x, out_rows, width), BF16),
                pltpu.VMEM((chunks, cross, out_rows, width), BF16),
                pltpu.VMEM((chunks, cross, out_rows, width), BF16),
                pltpu.VMEM((chunks, out_rows, width), F32),
                pltpu.VMEM((max(len(detours), 1), out_rows, width), BF16),
                pltpu.VMEM((HEAD, span), BF16),
                pltpu.VMEM((2, 1, span), F32),
                pltpu.VMEM((max(direct, 1), 2, out_rows, width), BF16),
                pltpu.VMEM((rows + 2 * WINDOW, span), F32),
                pltpu.SemaphoreType.DMA((4 * kvh + 2 * kvh * group + 5,)),
                pltpu.SemaphoreType.DMA((2, n, kvh, 2)),
                pltpu.SemaphoreType.DMA((n, kvh, 2)),
                pltpu.SemaphoreType.DMA((2,)),
                pltpu.SemaphoreType.DMA((2,)),
                pltpu.SemaphoreType.DMA((chunks,)),
                pltpu.SemaphoreType.DMA((chunks,)),
                pltpu.SemaphoreType.DMA((chunks, cross)),
                pltpu.SemaphoreType.DMA((chunks, cross)),
                pltpu.SemaphoreType.DMA((max(len(detours), 1),)),
                pltpu.SemaphoreType.DMA((max(len(detours), 1),)),
                pltpu.SemaphoreType.DMA((3,)),
                pltpu.SemaphoreType.DMA((3,)),
                pltpu.SemaphoreType.DMA((max(direct, 1), 2)),
                pltpu.SemaphoreType.DMA((max(direct, 1), 2)),
            ],
            compiler_params=pltpu.CompilerParams(
                collective_id=0, has_side_effects=True, vmem_limit_bytes=60 * 1024 * 1024
            ),
            name="hybrid",
        )(wq, wk, wv, gq, gk, gv, sink, qgain.reshape(1, HEAD), kgain.reshape(1, HEAD), ww, gw)

    return jax.shard_map(
        per_device,
        mesh=mesh,
        in_specs=(P(("grp", "sp"), "tp"),) * 6 + (P("tp"), P(), P(), P("tp", None), P("tp", None)),
        out_specs=P(("grp", "sp", "tp"), None),
        check_vma=False,
    )
```

```python
import functools
import math

import jax
import jax.numpy as jnp
from jax import lax
from jax.experimental import pallas as pl
from jax.experimental.pallas import tpu as pltpu
from jax.sharding import PartitionSpec as P

HEAD = 128
QH_A = 16
WINDOW = 128
GRID_W = 64
THETA = 10000.0
AWAY = 1e30
EPSILON = 1e-06
DIRECT = 128
LEND = True
MESH = pl.DeviceIdType.MESH
F32 = jnp.float32
BF16 = jnp.bfloat16


def dot_nt(a, b):
    return lax.dot_general(a, b, (((1,), (1,)), ((), ())), preferred_element_type=F32)


def dot_tn(a, b):
    return lax.dot_general(a, b, (((0,), (0,)), ((), ())), preferred_element_type=F32)


def kernel(
    n, n_tp, rows, kvh, group, cuts, direct, detours, lend,
    wq_hbm, wk_hbm, wv_hbm, gq_hbm, gk_hbm, gv_hbm, sink_hbm, qgain_hbm, kgain_hbm, ww_hbm, gw_hbm,
    out_ref,
    sink_ref, qgain_ref, kgain_ref, qw, wkv, qraw, kraw, qg, kvbuf, ww, gw, cosine, sine, top, total, acc, attn, proj, pbuf, dbuf, sbuf, rbuf, own, detour, lent, lent_sums, xbuf, far,
    lsem, gsend, grecv, hsend, hrecv, dsend, drecv, xsend, xrecv, rsend, rrecv, lsend, lrecv, usend, urecv,
):
    me = lax.axis_index("sp")
    t = lax.axis_index("tp")
    core = lax.rem(t, 2)
    x = t // 2
    n_x = n_tp // 2
    partner = x * 2 + 1 - core
    out_rows = rows // n_tp
    chunks = len(cuts)
    span = group * rows
    spans = [slice(begin, end) for begin, end in cuts]
    sizes = [slice(0, end - begin) for begin, end in cuts]
    has_left = me > 0
    has_right = me < n - 1
    at_end = jnp.logical_not(has_left & has_right)
    beside_end = (me == 1) | (me == n - 2)
    inner = jnp.where(me == 0, 1, n - 2)
    outer = jnp.where(me == 1, 0, n - 1)
    last = kvh - 1
    near = jnp.where(me >= n // 2, 0, 1)

    barrier = pltpu.get_barrier_semaphore()

    def greet(device):
        pl.semaphore_signal(barrier, inc=1, device_id=device, device_id_type=MESH)

    @pl.when(has_left)
    def _():
        greet({"sp": me - 1})

    @pl.when(has_right)
    def _():
        greet({"sp": me + 1})

    greet({"tp": partner})
    for dx in range(1, n_x):
        greet({"tp": lax.rem(x + dx, n_x) * 2 + core})
    if direct:
        greet({"tp": lax.rem(x + 1, n_x) * 2 + 1 - core})
    if detours:
        across = lax.rem(x + 1, n_x) * 2 + core

        @pl.when(at_end)
        def _():
            greet({"sp": inner, "tp": across})

        @pl.when(beside_end)
        def _():
            greet({"sp": outer, "tp": across})

    loads = []

    def load(src, dst):
        copy = pltpu.make_async_copy(src, dst, lsem.at[len(loads)])
        copy.start()
        loads.append(copy)
        return copy

    def head_cols(h):
        return slice(h * HEAD, (h + 1) * HEAD)

    v_loads = [load(gv_hbm.at[:, head_cols(g)], kvbuf.at[me, g, 1]) for g in range(kvh)]
    k_loads = [load(gk_hbm.at[:, head_cols(g)], kraw.at[g]) for g in range(kvh)]
    kgain_load = load(kgain_hbm, kgain_ref)
    qgain_load = load(qgain_hbm, qgain_ref)
    sink_load = load(sink_hbm, sink_ref)
    w_loads = []
    for g in range(kvh):
        w_loads.append(load(wk_hbm.at[:, head_cols(g)], wkv.at[g, 0, WINDOW : WINDOW + rows]))
        w_loads.append(load(wv_hbm.at[:, head_cols(g)], wkv.at[g, 1, WINDOW : WINDOW + rows]))
    q_loads = []
    for g in range(kvh):
        for u in range(group):
            q_loads.append(load(gq_hbm.at[:, head_cols(g * group + u)], qraw.at[g, u * rows : (u + 1) * rows]))
    wq_loads = []
    for g in range(kvh):
        for u in range(group):
            wq_loads.append(load(wq_hbm.at[:, head_cols(g * group + u)], qw.at[g, u * rows : (u + 1) * rows]))
    ww_load = load(ww_hbm, ww)
    gw_load = load(gw_hbm, gw)

    section = HEAD // 2
    half = section // 2

    def angles(row_place, column_place, shape):
        lane = lax.broadcasted_iota(jnp.int32, shape, 1)
        frequency = jnp.exp(jnp.bitwise_and(lane, half - 1).astype(F32) * (-2.0 * math.log(THETA) / section))
        return jnp.where(lane < section, row_place, column_place).astype(F32) * frequency

    def signed_sine(angle):
        low = jnp.bitwise_and(lax.broadcasted_iota(jnp.int32, angle.shape, 1), section - 1) < half
        return jnp.where(low, -jnp.sin(angle), jnp.sin(angle))

    def make_tables():
        if rows % GRID_W:
            place = me * rows + lax.broadcasted_iota(jnp.int32, (rows, HEAD), 0)
            angle = angles(place // GRID_W, lax.rem(place, GRID_W), (rows, HEAD))
            cosine[...] = jnp.cos(angle)
            sine[...] = signed_sine(angle)
            return
        lines = rows // GRID_W
        shape = (-(-lines // 8) * 8, HEAD)
        line = me * lines + lax.broadcasted_iota(jnp.int32, shape, 0)
        row_angle = angles(line, line, shape)
        column = lax.broadcasted_iota(jnp.int32, (GRID_W, HEAD), 0)
        column_angle = angles(column, column, (GRID_W, HEAD))
        by_row = lax.broadcasted_iota(jnp.int32, (GRID_W, HEAD), 1) < section
        for table, of in ((cosine, jnp.cos), (sine, signed_sine)):
            per_row, per_column = of(row_angle), of(column_angle)
            for r in range(lines):
                table[r * GRID_W : (r + 1) * GRID_W] = jnp.where(by_row, per_row[r : r + 1], per_column)

    def turn(values, gain):
        v = values.astype(F32)
        v = v * lax.rsqrt(jnp.mean(v * v, axis=1, keepdims=True) + EPSILON) * gain
        first = lax.broadcasted_iota(jnp.int32, v.shape, 1)
        other = jnp.where(
            jnp.bitwise_and(first, section - 1) < half,
            pltpu.roll(v, HEAD - half, 1),
            pltpu.roll(v, half, 1),
        )
        return (v * cosine[...] + other * sine[...]).astype(BF16)

    def block_copy(source, g, part, way):
        return pltpu.make_async_remote_copy(
            src_ref=kvbuf.at[source, g, part],
            dst_ref=kvbuf.at[source, g, part],
            send_sem=gsend.at[way, source, g, part],
            recv_sem=grecv.at[source, g, part],
            device_id={"sp": me + 1 - 2 * way},
            device_id_type=MESH,
        )

    def spread(g, part):
        kept = lend and g == last

        @pl.when((me < n - 2) if kept else has_right)
        def _():
            block_copy(me, g, part, 0).start()

        @pl.when((me > 1) if kept else has_left)
        def _():
            block_copy(me, g, part, 1).start()

    def lend_queries():
        return pltpu.make_async_remote_copy(
            src_ref=qg.at[last],
            dst_ref=qg.at[kvh],
            send_sem=lsend.at[0],
            recv_sem=lrecv.at[0],
            device_id={"sp": inner},
            device_id_type=MESH,
        )

    def return_lent():
        return [
            pltpu.make_async_remote_copy(
                src_ref=ref,
                dst_ref=ref,
                send_sem=lsend.at[1 + i],
                recv_sem=lrecv.at[1 + i],
                device_id={"sp": outer},
                device_id_type=MESH,
            )
            for i, ref in enumerate((lent, lent_sums))
        ]

    def halo_copy(direction):
        source = rows if direction == 0 else WINDOW
        target = 0 if direction == 0 else WINDOW + rows
        return pltpu.make_async_remote_copy(
            src_ref=wkv.at[:, :, source : source + WINDOW],
            dst_ref=wkv.at[:, :, target : target + WINDOW],
            send_sem=hsend.at[direction],
            recv_sem=hrecv.at[direction],
            device_id={"sp": me + 1 if direction == 0 else me - 1},
            device_id_type=MESH,
        )

    def start_halos():
        @pl.when(has_right)
        def _():
            halo_copy(0).start()

        @pl.when(has_left)
        def _():
            halo_copy(1).start()

    def turn_queries(g):
        for u in range(group):
            q_loads[g * group + u].wait()
        for u in range(group):
            part = slice(u * rows, (u + 1) * rows)
            qg[g, part] = turn(qraw[g, part], qgain_ref[...])

    make_tables()
    for copy in v_loads:
        copy.wait()
    greeted = has_left.astype(jnp.int32) + has_right.astype(jnp.int32) + n_x + (1 if direct else 0)
    if detours:
        greeted = greeted + at_end.astype(jnp.int32) + beside_end.astype(jnp.int32)
    pl.semaphore_wait(barrier, greeted)
    spread(0, 1)
    if lend:
        qgain_load.wait()
        turn_queries(last)

        @pl.when(at_end)
        def _():
            lend_queries().start()

    for g in range(1, kvh):
        spread(g, 1)
    for copy in w_loads:
        copy.wait()
    if lend:
        @pl.when(at_end)
        def _():
            start_halos()

    kgain_load.wait()
    for g in range(kvh):
        k_loads[g].wait()
        kvbuf[me, g, 0] = turn(kraw[g], kgain_ref[...])
        spread(g, 0)
    if lend:
        @pl.when(jnp.logical_not(at_end))
        def _():
            start_halos()
    else:
        start_halos()

    @pl.when(jnp.logical_not(has_left))
    def _():
        wkv[:, :, 0:WINDOW] = jnp.zeros((kvh, 2, WINDOW, HEAD), BF16)

    @pl.when(jnp.logical_not(has_right))
    def _():
        wkv[:, :, WINDOW + rows :] = jnp.zeros((kvh, 2, WINDOW, HEAD), BF16)

    if not lend:
        qgain_load.wait()
    for g in range(kvh - 1 if lend else kvh):
        turn_queries(g)

    scale = HEAD ** (-0.5)

    def absorb(source, g, first=False, slot=None):
        slot = g if slot is None else slot
        scores = dot_nt(kvbuf[source, g, 0], qg[slot]) * scale
        block_top = jnp.max(scores, axis=0, keepdims=True)
        if first:
            raised = jnp.exp(scores - block_top)
            top[slot] = block_top
            total[slot] = jnp.sum(raised, axis=0, keepdims=True)
            acc[slot] = dot_tn(kvbuf[source, g, 1], raised.astype(BF16))
        else:
            before = top[slot]
            new_top = jnp.maximum(before, block_top)
            fading = jnp.exp(before - new_top)
            raised = jnp.exp(scores - new_top)
            top[slot] = new_top
            total[slot] = total[slot] * fading + jnp.sum(raised, axis=0, keepdims=True)
            acc[slot] = acc[slot] * fading + dot_tn(kvbuf[source, g, 1], raised.astype(BF16))

    for g in range(kvh):
        absorb(me, g, True)

    def there(d, way, g):
        source = me - (1 - 2 * way) * d
        comes = (source >= 0) & (source < n)
        if lend and g == last and isinstance(d, int) and d <= 2:
            comes = comes & jnp.logical_not(at_end)
        return source, comes

    def piece(d, way, g, part):
        source, comes = there(d, way, g)
        target = me + 1 - 2 * way

        @pl.when(comes)
        def _():
            block_copy(source, g, part, way).wait_recv()
            kept = lend and g == last and isinstance(d, int) and d <= 1
            goes = (target > 0) & (target < n - 1) if kept else (target >= 0) & (target < n)

            @pl.when(goes)
            def _():
                block_copy(source, g, part, way).start()

    def take(d, way, g):
        source, comes = there(d, way, g)

        @pl.when(comes)
        def _():
            absorb(source, g)

    def take_all(d, way):
        if lend and d <= 2:
            source = me - (1 - 2 * way) * d
            inside = (source >= 0) & (source < n)

            @pl.when(inside & jnp.logical_not(at_end))
            def _():
                for g in range(kvh):
                    absorb(source, g)

            @pl.when(inside & at_end)
            def _():
                for g in range(last):
                    absorb(source, g)
        else:
            source, comes = there(d, way, 0)

            @pl.when(comes)
            def _():
                for g in range(kvh):
                    absorb(source, g)

    def relay_near():
        far_way = 1 - near
        for g in range(kvh):
            piece(1, near, g, 1)
        piece(1, far_way, 0, 1)
        for g in range(kvh):
            if lend and g == last:
                @pl.when(beside_end)
                def _():
                    lend_queries().wait_recv()
                    absorb(me, last, True, kvh)

            piece(1, near, g, 0)
        if lend:
            @pl.when(beside_end)
            def _():
                absorb(there(1, near, last)[0], last, False, kvh)
                lent[...] = (acc[kvh] * (1.0 / total[kvh])).astype(BF16)
                lent_sums[0] = top[kvh]
                lent_sums[1] = total[kvh]
                for copy in return_lent():
                    copy.start()

        for g in range(1, kvh):
            piece(1, far_way, g, 1)
        take_all(1, near)

    def relay(d):
        ways = [near, 1 - near] if not isinstance(d, int) or d < n - n // 2 else [near]
        for part in (1, 0):
            for g in range(kvh):
                for way in ways:
                    piece(d, way, g, part)
                if part == 0:
                    for way in ways:
                        take(d, way, g)
                    if n == 4:
                        @pl.when(at_end)
                        def _():
                            finish(g)

    def relay_far_and_second():
        other = 1 - near
        ways = (near, other)[: 2 if n > 4 else 1]

        def second(g, part):
            for way in ways if n > 2 else ():
                piece(2, way, g, part)

        def take_second(g):
            for way in ways if n > 2 else ():
                take(2, way, g)

        window_head(0)
        piece(1, other, 0, 0)
        second(0, 1)
        for g in range(1, kvh):
            window_head(g)
        take(1, other, 0)
        for g in range(1, kvh):
            piece(1, other, g, 0)
            second(g, 1)
            take(1, other, g)
        window_project(0, chunks)
        for g in range(kvh):
            second(g, 0)
            take_second(g)
            if n == 4:
                @pl.when(jnp.logical_not(at_end))
                def _():
                    finish(g)

    def merge_lent():
        for copy in return_lent():
            copy.wait_recv()
        before = top[last]
        new_top = jnp.maximum(before, lent_sums[0])
        fading = jnp.exp(before - new_top)
        share = jnp.exp(lent_sums[0] - new_top) * lent_sums[1]
        top[last] = new_top
        total[last] = total[last] * fading + share
        acc[last] = acc[last] * fading + lent[...].astype(F32) * share

    def put_heads(base, g, value):
        turned = jnp.transpose(value).astype(BF16)
        for u in range(group):
            attn[:, base + (g * group + u) * HEAD : base + (g * group + u + 1) * HEAD] = turned[u * rows : (u + 1) * rows]

    heads_width = kvh * group * HEAD

    def finish(g):
        put_heads(heads_width, g, acc[g] * (1.0 / total[g]))

    def window_inputs():
        sink_load.wait()
        for copy in wq_loads:
            copy.wait()

        @pl.when(has_left)
        def _():
            halo_copy(0).wait_recv()

        @pl.when(has_right)
        def _():
            halo_copy(1).wait_recv()

    padded = rows + 2 * WINDOW

    def make_distances():
        key_at = lax.broadcasted_iota(jnp.int32, (padded, span), 0) - WINDOW
        column = lax.broadcasted_iota(jnp.int32, (1, span), 1)
        distance = jnp.abs(key_at - lax.rem(column, rows))
        key_place = me * rows + lax.broadcasted_iota(jnp.int32, (padded, 1), 0) - WINDOW
        reach = jnp.where((key_place >= 0) & (key_place < n * rows), WINDOW, -1)
        far[...] = jnp.where(distance <= reach, distance.astype(F32), AWAY)

    def window_head(g):
        if g == 0:
            window_inputs()
        member = lax.broadcasted_iota(jnp.int32, (1, span), 1) // rows
        head = (t * (kvh * group) + g * group + 1 + member).astype(F32)
        slope = jnp.exp2(head * (-8.0 / QH_A))
        sink = jnp.zeros((1, span), F32)
        for u in range(group):
            sink = jnp.where(member == u, sink_ref[g * group + u], sink)
        scores = dot_nt(wkv[g, 0], qw[g]) * scale
        scores = scores - slope * far[...]
        highest = jnp.maximum(jnp.max(scores, axis=0, keepdims=True), sink)
        raised = jnp.exp(scores - highest)
        bottom = jnp.sum(raised, axis=0, keepdims=True) + jnp.exp(sink - highest)
        weights = (raised * (1.0 / bottom)).astype(BF16)
        put_heads(0, g, dot_tn(wkv[g, 1], weights))

    def window_project(begin, end):
        if begin == 0:
            ww_load.wait()
        for j in range(begin, end):
            cols = spans[j]
            proj[:, cols] = jnp.dot(attn[:, :heads_width], ww[:, cols], preferred_element_type=F32)

    make_distances()
    if n > 1:
        relay_near()
    if n > 1:
        relay_far_and_second()
    else:
        for g in range(kvh):
            window_head(g)
        window_project(0, chunks)
    if lend:
        @pl.when(at_end)
        def _():
            merge_lent()

    if n <= 4:
        for d in range(3, n):
            relay(d)
    else:
        def relay_step(d, carry):
            relay(d)
            return carry

        lax.fori_loop(3, n, relay_step, 0)

    if n != 4:
        for g in range(kvh):
            finish(g)
    gw_load.wait()

    def pair_copy(j):
        return pltpu.make_async_remote_copy(
            src_ref=pbuf.at[j, 1 - core, :, :, sizes[j]],
            dst_ref=dbuf.at[j, :, :, sizes[j]],
            send_sem=dsend.at[j],
            recv_sem=drecv.at[j],
            device_id={"tp": partner},
            device_id_type=MESH,
        )

    def cross_copy(j, dx):
        return pltpu.make_async_remote_copy(
            src_ref=sbuf.at[j, dx - 1, :, sizes[j]],
            dst_ref=rbuf.at[j, dx - 1, :, sizes[j]],
            send_sem=xsend.at[j, dx - 1],
            recv_sem=xrecv.at[j, dx - 1],
            device_id={"tp": lax.rem(x + dx, n_x) * 2 + core},
            device_id_type=MESH,
        )

    def direct_pair_copy(j):
        return pltpu.make_async_remote_copy(
            src_ref=pbuf.at[j, 1 - core, x, :, sizes[j]],
            dst_ref=dbuf.at[j, x, :, sizes[j]],
            send_sem=dsend.at[j],
            recv_sem=drecv.at[j],
            device_id={"tp": partner},
            device_id_type=MESH,
        )

    def direct_copy(j, flip):
        to = core if flip == 0 else 1 - core
        return pltpu.make_async_remote_copy(
            src_ref=pbuf.at[j, to, lax.rem(x + 1, n_x), :, sizes[j]],
            dst_ref=xbuf.at[j, flip, :, sizes[j]],
            send_sem=usend.at[j, flip],
            recv_sem=urecv.at[j, flip],
            device_id={"tp": lax.rem(x + 1, n_x) * 2 + to},
            device_id_type=MESH,
        )

    def detour_copy(j):
        return pltpu.make_async_remote_copy(
            src_ref=sbuf.at[j, 0, :, sizes[j]],
            dst_ref=detour.at[detours.index(j), :, sizes[j]],
            send_sem=xsend.at[j, 0],
            recv_sem=rrecv.at[detours.index(j)],
            device_id={"sp": inner, "tp": across},
            device_id_type=MESH,
        )

    def detour_end_copy(j):
        return pltpu.make_async_remote_copy(
            src_ref=detour.at[detours.index(j), :, sizes[j]],
            dst_ref=rbuf.at[j, 0, :, sizes[j]],
            send_sem=rsend.at[detours.index(j)],
            recv_sem=xrecv.at[j, 0],
            device_id={"sp": outer},
            device_id_type=MESH,
        )

    def pass_on(j):
        pair_copy(j).wait_recv()
        for dx in range(1, n_x):
            other = lax.rem(x + dx, n_x)
            both = pbuf[j, core, other, :, sizes[j]].astype(F32) + dbuf[j, other, :, sizes[j]].astype(F32)
            sbuf[j, dx - 1, :, sizes[j]] = both.astype(BF16)
            if j in detours:
                @pl.when(at_end)
                def _():
                    detour_copy(j).start()

                @pl.when(jnp.logical_not(at_end))
                def _():
                    cross_copy(j, dx).start()
            else:
                cross_copy(j, dx).start()
        own[j, :, sizes[j]] = pbuf[j, core, x, :, sizes[j]].astype(F32) + dbuf[j, x, :, sizes[j]].astype(F32)

    def project(j):
        part = proj[:, spans[j]] + jnp.dot(attn[:, heads_width:], gw[:, spans[j]], preferred_element_type=F32)
        for b in range(n_tp):
            pbuf[j, b % 2, b // 2, :, sizes[j]] = part[b * out_rows : (b + 1) * out_rows].astype(BF16)
        if j < direct:
            direct_pair_copy(j).start()
            for c in range(2):
                direct_copy(j, c).start()
        else:
            pair_copy(j).start()

    for j in range(direct + 1):
        project(j)
    project(direct + 1)
    pass_on(direct)
    for j in range(direct + 2, chunks):
        project(j)
        if j > direct + 2:
            pass_on(j - 2)
    for j in range(chunks - 2, chunks):
        pass_on(j)

    for j in detours:
        @pl.when(beside_end)
        def _():
            detour_copy(j).wait_recv()
            detour_end_copy(j).start()

    for j in range(direct):
        direct_pair_copy(j).wait()
        for c in range(2):
            direct_copy(j, c).wait()
        value = pbuf[j, core, x, :, sizes[j]].astype(F32) + dbuf[j, x, :, sizes[j]].astype(F32)
        for c in range(2):
            value = value + xbuf[j, c, :, sizes[j]].astype(F32)
        out_ref[:, spans[j]] = value.astype(BF16)
    for j in range(direct, chunks):
        value = own[j, :, sizes[j]]
        for dx in range(1, n_x):
            cross_copy(j, dx).wait_recv()
            value = value + rbuf[j, dx - 1, :, sizes[j]].astype(F32)
        out_ref[:, spans[j]] = value.astype(BF16)

    for j in range(direct, chunks):
        pair_copy(j).wait_send()
        for dx in range(1, n_x):
            cross_copy(j, dx).wait_send()
    for j in detours:
        @pl.when(beside_end)
        def _():
            detour_end_copy(j).wait_send()

    @pl.when(has_right)
    def _():
        halo_copy(0).wait_send()

    @pl.when(has_left)
    def _():
        halo_copy(1).wait_send()

    if lend:
        @pl.when(at_end)
        def _():
            lend_queries().wait_send()

        @pl.when(beside_end)
        def _():
            for copy in return_lent():
                copy.wait_send()

    def drain(source, carry):
        for g in range(kvh):
            right = has_right & (source <= me)
            left = has_left & (source >= me)
            if lend and g == last:
                right = right & jnp.logical_not((me == n - 2) & (source >= n - 3))
                left = left & jnp.logical_not((me == 1) & (source <= 2))
            for part in range(2):
                @pl.when(right)
                def _():
                    block_copy(source, g, part, 0).wait_send()

                @pl.when(left)
                def _():
                    block_copy(source, g, part, 1).wait_send()

        return carry

    lax.fori_loop(0, n, drain, 0)


def solution(mesh):
    n, n_tp = mesh.shape["sp"], mesh.shape["tp"]

    def per_device(wq, wk, wv, gq, gk, gv, sink, qgain, kgain, ww, gw):
        rows = wq.shape[0]
        kvh = wk.shape[1] // HEAD
        group = wq.shape[1] // wk.shape[1]
        model = ww.shape[1]
        chunks = 8
        width = model // chunks
        cuts = [(j * width, (j + 1) * width) for j in range(chunks)]
        direct = 0
        n_x = n_tp // 2
        out_rows = rows // n_tp
        heads_width = kvh * group * HEAD
        span = group * rows
        if n_tp == 4 and model % 4096 == 0:
            direct = 1
            edges = [0]
            for part in (1, 3, 4, 5, 4, 4, 4, 4, 3):
                edges.append(edges[-1] + part * model // 32)
            cuts = list(zip(edges[:-1], edges[1:]))
            width = max(end - begin for begin, end in cuts)
        chunks = len(cuts)
        any_spec = pl.BlockSpec(memory_space=pl.ANY)
        vmem = pl.BlockSpec(memory_space=pltpu.VMEM)
        cross = max(n_x - 1, 1)
        lend = LEND and n >= 4 and kvh >= 2
        detours = (3,) if n >= 4 and n_x == 2 else ()
        return pl.pallas_call(
            functools.partial(kernel, n, n_tp, rows, kvh, group, cuts, direct, detours, lend),
            out_shape=pltpu.VMEM((out_rows, model), BF16),
            in_specs=[any_spec] * 11,
            out_specs=vmem,
            scratch_shapes=[
                pltpu.SMEM(sink.shape, F32),
                pltpu.VMEM((1, HEAD), F32),
                pltpu.VMEM((1, HEAD), F32),
                pltpu.VMEM((kvh, span, HEAD), BF16),
                pltpu.VMEM((kvh, 2, rows + 2 * WINDOW, HEAD), BF16),
                pltpu.VMEM((kvh, span, HEAD), BF16),
                pltpu.VMEM((kvh, rows, HEAD), BF16),
                pltpu.VMEM((kvh + lend, span, HEAD), BF16),
                pltpu.VMEM((n, kvh, 2, rows, HEAD), BF16),
                pltpu.VMEM(ww.shape, BF16),
                pltpu.VMEM(gw.shape, BF16),
                pltpu.VMEM((rows, HEAD), F32),
                pltpu.VMEM((rows, HEAD), F32),
                pltpu.VMEM((kvh + lend, 1, span), F32),
                pltpu.VMEM((kvh + lend, 1, span), F32),
                pltpu.VMEM((kvh + lend, HEAD, span), F32),
                pltpu.VMEM((rows, 2 * heads_width), BF16),
                pltpu.VMEM((rows, model), F32),
                pltpu.VMEM((chunks, 2, n_x, out_rows, width), BF16),
                pltpu.VMEM((chunks, n_x, out_rows, width), BF16),
                pltpu.VMEM((chunks, cross, out_rows, width), BF16),
                pltpu.VMEM((chunks, cross, out_rows, width), BF16),
                pltpu.VMEM((chunks, out_rows, width), F32),
                pltpu.VMEM((max(len(detours), 1), out_rows, width), BF16),
                pltpu.VMEM((HEAD, span), BF16),
                pltpu.VMEM((2, 1, span), F32),
                pltpu.VMEM((max(direct, 1), 2, out_rows, width), BF16),
                pltpu.VMEM((rows + 2 * WINDOW, span), F32),
                pltpu.SemaphoreType.DMA((4 * kvh + 2 * kvh * group + 5,)),
                pltpu.SemaphoreType.DMA((2, n, kvh, 2)),
                pltpu.SemaphoreType.DMA((n, kvh, 2)),
                pltpu.SemaphoreType.DMA((2,)),
                pltpu.SemaphoreType.DMA((2,)),
                pltpu.SemaphoreType.DMA((chunks,)),
                pltpu.SemaphoreType.DMA((chunks,)),
                pltpu.SemaphoreType.DMA((chunks, cross)),
                pltpu.SemaphoreType.DMA((chunks, cross)),
                pltpu.SemaphoreType.DMA((max(len(detours), 1),)),
                pltpu.SemaphoreType.DMA((max(len(detours), 1),)),
                pltpu.SemaphoreType.DMA((3,)),
                pltpu.SemaphoreType.DMA((3,)),
                pltpu.SemaphoreType.DMA((max(direct, 1), 2)),
                pltpu.SemaphoreType.DMA((max(direct, 1), 2)),
            ],
            compiler_params=pltpu.CompilerParams(
                collective_id=0, has_side_effects=True, vmem_limit_bytes=60 * 1024 * 1024
            ),
            name="hybrid",
        )(wq, wk, wv, gq, gk, gv, sink, qgain.reshape(1, HEAD), kgain.reshape(1, HEAD), ww, gw)

    return jax.shard_map(
        per_device,
        mesh=mesh,
        in_specs=(P(("grp", "sp"), "tp"),) * 6 + (P("tp"), P(), P(), P("tp", None), P("tp", None)),
        out_specs=P(("grp", "sp", "tp"), None),
        check_vma=False,
    )
```

```python
import functools
import math

import jax
import jax.numpy as jnp
from jax import lax
from jax.experimental import pallas as pl
from jax.experimental.pallas import tpu as pltpu
from jax.sharding import PartitionSpec as P

HEAD = 128
QH_A = 16
WINDOW = 128
GRID_W = 64
THETA = 10000.0
AWAY = 1e30
LOG2E = math.log2(math.e)
EPSILON = 1e-06
DIRECT = 128
LEND = True
MESH = pl.DeviceIdType.MESH
F32 = jnp.float32
BF16 = jnp.bfloat16


def dot_nt(a, b):
    return lax.dot_general(a, b, (((1,), (1,)), ((), ())), preferred_element_type=F32)


def dot_tn(a, b):
    return lax.dot_general(a, b, (((0,), (0,)), ((), ())), preferred_element_type=F32)


def kernel(
    n, n_tp, rows, kvh, group, cuts, direct, detours, lend,
    wq_hbm, wk_hbm, wv_hbm, gq_hbm, gk_hbm, gv_hbm, sink_hbm, qgain_hbm, kgain_hbm, ww_hbm, gw_hbm,
    out_ref,
    sink_ref, qgain_ref, kgain_ref, qw, wkv, qraw, kraw, qg, kvbuf, ww, gw, cosine, sine, top, total, acc, attn, proj, pbuf, dbuf, sbuf, rbuf, own, detour, lent, lent_sums, xbuf, far,
    lsem, gsend, grecv, hsend, hrecv, dsend, drecv, xsend, xrecv, rsend, rrecv, lsend, lrecv, usend, urecv,
):
    me = lax.axis_index("sp")
    t = lax.axis_index("tp")
    core = lax.rem(t, 2)
    x = t // 2
    n_x = n_tp // 2
    partner = x * 2 + 1 - core
    out_rows = rows // n_tp
    chunks = len(cuts)
    span = group * rows
    spans = [slice(begin, end) for begin, end in cuts]
    sizes = [slice(0, end - begin) for begin, end in cuts]
    has_left = me > 0
    has_right = me < n - 1
    at_end = jnp.logical_not(has_left & has_right)
    beside_end = (me == 1) | (me == n - 2)
    inner = jnp.where(me == 0, 1, n - 2)
    outer = jnp.where(me == 1, 0, n - 1)
    last = kvh - 1
    near = jnp.where(me >= n // 2, 0, 1)

    barrier = pltpu.get_barrier_semaphore()

    def greet(device):
        pl.semaphore_signal(barrier, inc=1, device_id=device, device_id_type=MESH)

    @pl.when(has_left)
    def _():
        greet({"sp": me - 1})

    @pl.when(has_right)
    def _():
        greet({"sp": me + 1})

    greet({"tp": partner})
    for dx in range(1, n_x):
        greet({"tp": lax.rem(x + dx, n_x) * 2 + core})
    if direct:
        greet({"tp": lax.rem(x + 1, n_x) * 2 + 1 - core})
    if detours:
        across = lax.rem(x + 1, n_x) * 2 + core

        @pl.when(at_end)
        def _():
            greet({"sp": inner, "tp": across})

        @pl.when(beside_end)
        def _():
            greet({"sp": outer, "tp": across})

    loads = []

    def load(src, dst):
        copy = pltpu.make_async_copy(src, dst, lsem.at[len(loads)])
        copy.start()
        loads.append(copy)
        return copy

    def head_cols(h):
        return slice(h * HEAD, (h + 1) * HEAD)

    v_loads = [load(gv_hbm.at[:, head_cols(g)], kvbuf.at[me, g, 1]) for g in range(kvh)]
    k_loads = [load(gk_hbm.at[:, head_cols(g)], kraw.at[g]) for g in range(kvh)]
    kgain_load = load(kgain_hbm, kgain_ref)
    qgain_load = load(qgain_hbm, qgain_ref)
    sink_load = load(sink_hbm, sink_ref)
    w_loads = []
    for g in range(kvh):
        w_loads.append(load(wk_hbm.at[:, head_cols(g)], wkv.at[g, 0, WINDOW : WINDOW + rows]))
        w_loads.append(load(wv_hbm.at[:, head_cols(g)], wkv.at[g, 1, WINDOW : WINDOW + rows]))
    q_loads = []
    for g in range(kvh):
        for u in range(group):
            q_loads.append(load(gq_hbm.at[:, head_cols(g * group + u)], qraw.at[g, u * rows : (u + 1) * rows]))
    wq_loads = []
    for g in range(kvh):
        for u in range(group):
            wq_loads.append(load(wq_hbm.at[:, head_cols(g * group + u)], qw.at[g, u * rows : (u + 1) * rows]))
    ww_load = load(ww_hbm, ww)
    gw_load = load(gw_hbm, gw)

    section = HEAD // 2
    half = section // 2

    def angles(row_place, column_place, shape):
        lane = lax.broadcasted_iota(jnp.int32, shape, 1)
        frequency = jnp.exp(jnp.bitwise_and(lane, half - 1).astype(F32) * (-2.0 * math.log(THETA) / section))
        return jnp.where(lane < section, row_place, column_place).astype(F32) * frequency

    def signed_sine(angle):
        low = jnp.bitwise_and(lax.broadcasted_iota(jnp.int32, angle.shape, 1), section - 1) < half
        return jnp.where(low, -jnp.sin(angle), jnp.sin(angle))

    def make_tables():
        if rows % GRID_W:
            place = me * rows + lax.broadcasted_iota(jnp.int32, (rows, HEAD), 0)
            angle = angles(place // GRID_W, lax.rem(place, GRID_W), (rows, HEAD))
            cosine[...] = jnp.cos(angle)
            sine[...] = signed_sine(angle)
            return
        lines = rows // GRID_W
        shape = (-(-lines // 8) * 8, HEAD)
        line = me * lines + lax.broadcasted_iota(jnp.int32, shape, 0)
        row_angle = angles(line, line, shape)
        column = lax.broadcasted_iota(jnp.int32, (GRID_W, HEAD), 0)
        column_angle = angles(column, column, (GRID_W, HEAD))
        by_row = lax.broadcasted_iota(jnp.int32, (GRID_W, HEAD), 1) < section
        for table, of in ((cosine, jnp.cos), (sine, signed_sine)):
            per_row, per_column = of(row_angle), of(column_angle)
            for r in range(lines):
                table[r * GRID_W : (r + 1) * GRID_W] = jnp.where(by_row, per_row[r : r + 1], per_column)

    def turn(values, gain):
        v = values.astype(F32)
        v = v * lax.rsqrt(jnp.mean(v * v, axis=1, keepdims=True) + EPSILON) * gain
        first = lax.broadcasted_iota(jnp.int32, v.shape, 1)
        other = jnp.where(
            jnp.bitwise_and(first, section - 1) < half,
            pltpu.roll(v, HEAD - half, 1),
            pltpu.roll(v, half, 1),
        )
        return (v * cosine[...] + other * sine[...]).astype(BF16)

    def block_copy(source, g, part, way):
        return pltpu.make_async_remote_copy(
            src_ref=kvbuf.at[source, g, part],
            dst_ref=kvbuf.at[source, g, part],
            send_sem=gsend.at[way, source, g, part],
            recv_sem=grecv.at[source, g, part],
            device_id={"sp": me + 1 - 2 * way},
            device_id_type=MESH,
        )

    def spread(g, part):
        kept = lend and g == last

        @pl.when((me < n - 2) if kept else has_right)
        def _():
            block_copy(me, g, part, 0).start()

        @pl.when((me > 1) if kept else has_left)
        def _():
            block_copy(me, g, part, 1).start()

    def lend_queries():
        return pltpu.make_async_remote_copy(
            src_ref=qg.at[last],
            dst_ref=qg.at[kvh],
            send_sem=lsend.at[0],
            recv_sem=lrecv.at[0],
            device_id={"sp": inner},
            device_id_type=MESH,
        )

    def return_lent():
        return [
            pltpu.make_async_remote_copy(
                src_ref=ref,
                dst_ref=ref,
                send_sem=lsend.at[1 + i],
                recv_sem=lrecv.at[1 + i],
                device_id={"sp": outer},
                device_id_type=MESH,
            )
            for i, ref in enumerate((lent, lent_sums))
        ]

    def halo_copy(direction):
        source = rows if direction == 0 else WINDOW
        target = 0 if direction == 0 else WINDOW + rows
        return pltpu.make_async_remote_copy(
            src_ref=wkv.at[:, :, source : source + WINDOW],
            dst_ref=wkv.at[:, :, target : target + WINDOW],
            send_sem=hsend.at[direction],
            recv_sem=hrecv.at[direction],
            device_id={"sp": me + 1 if direction == 0 else me - 1},
            device_id_type=MESH,
        )

    def start_halos():
        @pl.when(has_right)
        def _():
            halo_copy(0).start()

        @pl.when(has_left)
        def _():
            halo_copy(1).start()

    def turn_queries(g):
        for u in range(group):
            q_loads[g * group + u].wait()
        for u in range(group):
            part = slice(u * rows, (u + 1) * rows)
            qg[g, part] = turn(qraw[g, part], qgain_ref[...])

    make_tables()
    for copy in v_loads:
        copy.wait()
    greeted = has_left.astype(jnp.int32) + has_right.astype(jnp.int32) + n_x + (1 if direct else 0)
    if detours:
        greeted = greeted + at_end.astype(jnp.int32) + beside_end.astype(jnp.int32)
    pl.semaphore_wait(barrier, greeted)
    spread(0, 1)
    if lend:
        qgain_load.wait()
        turn_queries(last)

        @pl.when(at_end)
        def _():
            lend_queries().start()

    for g in range(1, kvh):
        spread(g, 1)
    for copy in w_loads:
        copy.wait()
    if lend:
        @pl.when(at_end)
        def _():
            start_halos()

    kgain_load.wait()
    for g in range(kvh):
        k_loads[g].wait()
        kvbuf[me, g, 0] = turn(kraw[g], kgain_ref[...])
        spread(g, 0)
    if lend:
        @pl.when(jnp.logical_not(at_end))
        def _():
            start_halos()
    else:
        start_halos()

    @pl.when(jnp.logical_not(has_left))
    def _():
        wkv[:, :, 0:WINDOW] = jnp.zeros((kvh, 2, WINDOW, HEAD), BF16)

    @pl.when(jnp.logical_not(has_right))
    def _():
        wkv[:, :, WINDOW + rows :] = jnp.zeros((kvh, 2, WINDOW, HEAD), BF16)

    if not lend:
        qgain_load.wait()
    for g in range(kvh - 1 if lend else kvh):
        turn_queries(g)

    scale = HEAD ** (-0.5) * LOG2E

    def absorb(source, g, first=False, slot=None):
        slot = g if slot is None else slot
        scores = dot_nt(kvbuf[source, g, 0], qg[slot]) * scale
        block_top = jnp.max(scores, axis=0, keepdims=True)
        if first:
            raised = jnp.exp2(scores - block_top)
            top[slot] = block_top
            total[slot] = jnp.sum(raised, axis=0, keepdims=True)
            acc[slot] = dot_tn(kvbuf[source, g, 1], raised.astype(BF16))
        else:
            before = top[slot]
            new_top = jnp.maximum(before, block_top)
            fading = jnp.exp2(before - new_top)
            raised = jnp.exp2(scores - new_top)
            top[slot] = new_top
            total[slot] = total[slot] * fading + jnp.sum(raised, axis=0, keepdims=True)
            acc[slot] = acc[slot] * fading + dot_tn(kvbuf[source, g, 1], raised.astype(BF16))

    for g in range(kvh):
        absorb(me, g, True)

    def there(d, way, g):
        source = me - (1 - 2 * way) * d
        comes = (source >= 0) & (source < n)
        if lend and g == last and isinstance(d, int) and d <= 2:
            comes = comes & jnp.logical_not(at_end)
        return source, comes

    def piece(d, way, g, part):
        source, comes = there(d, way, g)
        target = me + 1 - 2 * way

        @pl.when(comes)
        def _():
            block_copy(source, g, part, way).wait_recv()
            kept = lend and g == last and isinstance(d, int) and d <= 1
            goes = (target > 0) & (target < n - 1) if kept else (target >= 0) & (target < n)

            @pl.when(goes)
            def _():
                block_copy(source, g, part, way).start()

    def take(d, way, g):
        source, comes = there(d, way, g)

        @pl.when(comes)
        def _():
            absorb(source, g)

    def take_all(d, way):
        if lend and d <= 2:
            source = me - (1 - 2 * way) * d
            inside = (source >= 0) & (source < n)

            @pl.when(inside & jnp.logical_not(at_end))
            def _():
                for g in range(kvh):
                    absorb(source, g)

            @pl.when(inside & at_end)
            def _():
                for g in range(last):
                    absorb(source, g)
        else:
            source, comes = there(d, way, 0)

            @pl.when(comes)
            def _():
                for g in range(kvh):
                    absorb(source, g)

    def relay_near():
        far_way = 1 - near
        for g in range(kvh):
            piece(1, near, g, 1)
        piece(1, far_way, 0, 1)
        for g in range(kvh):
            if lend and g == last:
                @pl.when(beside_end)
                def _():
                    lend_queries().wait_recv()
                    absorb(me, last, True, kvh)

            piece(1, near, g, 0)
        if lend:
            @pl.when(beside_end)
            def _():
                absorb(there(1, near, last)[0], last, False, kvh)
                lent[...] = (acc[kvh] * (1.0 / total[kvh])).astype(BF16)
                lent_sums[0] = top[kvh]
                lent_sums[1] = total[kvh]
                for copy in return_lent():
                    copy.start()

        for g in range(1, kvh):
            piece(1, far_way, g, 1)
        take_all(1, near)

    def relay(d):
        ways = [near, 1 - near] if not isinstance(d, int) or d < n - n // 2 else [near]
        for part in (1, 0):
            for g in range(kvh):
                for way in ways:
                    piece(d, way, g, part)
                if part == 0:
                    for way in ways:
                        take(d, way, g)
                    if n == 4:
                        @pl.when(at_end)
                        def _():
                            finish(g)

    def relay_far_and_second():
        other = 1 - near
        ways = (near, other)[: 2 if n > 4 else 1]

        def second(g, part):
            for way in ways if n > 2 else ():
                piece(2, way, g, part)

        def take_second(g):
            for way in ways if n > 2 else ():
                take(2, way, g)

        window_head(0)
        piece(1, other, 0, 0)
        second(0, 1)
        for g in range(1, kvh):
            window_head(g)
        take(1, other, 0)
        for g in range(1, kvh):
            piece(1, other, g, 0)
            second(g, 1)
            take(1, other, g)
        window_project(0, chunks)
        for g in range(kvh):
            second(g, 0)
            take_second(g)
            if n == 4:
                @pl.when(jnp.logical_not(at_end))
                def _():
                    finish(g)

    def merge_lent():
        for copy in return_lent():
            copy.wait_recv()
        before = top[last]
        new_top = jnp.maximum(before, lent_sums[0])
        fading = jnp.exp2(before - new_top)
        share = jnp.exp2(lent_sums[0] - new_top) * lent_sums[1]
        top[last] = new_top
        total[last] = total[last] * fading + share
        acc[last] = acc[last] * fading + lent[...].astype(F32) * share

    def put_heads(base, g, value):
        turned = jnp.transpose(value).astype(BF16)
        for u in range(group):
            attn[:, base + (g * group + u) * HEAD : base + (g * group + u + 1) * HEAD] = turned[u * rows : (u + 1) * rows]

    heads_width = kvh * group * HEAD

    def finish(g):
        put_heads(heads_width, g, acc[g] * (1.0 / total[g]))

    def window_inputs():
        sink_load.wait()
        for copy in wq_loads:
            copy.wait()

        @pl.when(has_left)
        def _():
            halo_copy(0).wait_recv()

        @pl.when(has_right)
        def _():
            halo_copy(1).wait_recv()

    padded = rows + 2 * WINDOW

    def make_distances():
        key_at = lax.broadcasted_iota(jnp.int32, (padded, span), 0) - WINDOW
        column = lax.broadcasted_iota(jnp.int32, (1, span), 1)
        distance = jnp.abs(key_at - lax.rem(column, rows))
        key_place = me * rows + lax.broadcasted_iota(jnp.int32, (padded, 1), 0) - WINDOW
        reach = jnp.where((key_place >= 0) & (key_place < n * rows), WINDOW, -1)
        far[...] = jnp.where(distance <= reach, distance.astype(F32), AWAY)

    def window_head(g):
        if g == 0:
            window_inputs()
        member = lax.broadcasted_iota(jnp.int32, (1, span), 1) // rows
        head = (t * (kvh * group) + g * group + 1 + member).astype(F32)
        slope = jnp.exp2(head * (-8.0 / QH_A)) * LOG2E
        sink = jnp.zeros((1, span), F32)
        for u in range(group):
            sink = jnp.where(member == u, sink_ref[g * group + u] * LOG2E, sink)
        scores = dot_nt(wkv[g, 0], qw[g]) * scale
        scores = scores - slope * far[...]
        highest = jnp.maximum(jnp.max(scores, axis=0, keepdims=True), sink)
        raised = jnp.exp2(scores - highest)
        bottom = jnp.sum(raised, axis=0, keepdims=True) + jnp.exp2(sink - highest)
        weights = (raised * (1.0 / bottom)).astype(BF16)
        put_heads(0, g, dot_tn(wkv[g, 1], weights))

    def window_project(begin, end):
        if begin == 0:
            ww_load.wait()
        for j in range(begin, end):
            cols = spans[j]
            proj[:, cols] = jnp.dot(attn[:, :heads_width], ww[:, cols], preferred_element_type=F32)

    make_distances()
    if n > 1:
        relay_near()
    if n > 1:
        relay_far_and_second()
    else:
        for g in range(kvh):
            window_head(g)
        window_project(0, chunks)
    if lend:
        @pl.when(at_end)
        def _():
            merge_lent()

    if n <= 4:
        for d in range(3, n):
            relay(d)
    else:
        def relay_step(d, carry):
            relay(d)
            return carry

        lax.fori_loop(3, n, relay_step, 0)

    if n != 4:
        for g in range(kvh):
            finish(g)
    gw_load.wait()

    def pair_copy(j):
        return pltpu.make_async_remote_copy(
            src_ref=pbuf.at[j, 1 - core, :, :, sizes[j]],
            dst_ref=dbuf.at[j, :, :, sizes[j]],
            send_sem=dsend.at[j],
            recv_sem=drecv.at[j],
            device_id={"tp": partner},
            device_id_type=MESH,
        )

    def cross_copy(j, dx):
        return pltpu.make_async_remote_copy(
            src_ref=sbuf.at[j, dx - 1, :, sizes[j]],
            dst_ref=rbuf.at[j, dx - 1, :, sizes[j]],
            send_sem=xsend.at[j, dx - 1],
            recv_sem=xrecv.at[j, dx - 1],
            device_id={"tp": lax.rem(x + dx, n_x) * 2 + core},
            device_id_type=MESH,
        )

    def direct_pair_copy(j):
        return pltpu.make_async_remote_copy(
            src_ref=pbuf.at[j, 1 - core, x, :, sizes[j]],
            dst_ref=dbuf.at[j, x, :, sizes[j]],
            send_sem=dsend.at[j],
            recv_sem=drecv.at[j],
            device_id={"tp": partner},
            device_id_type=MESH,
        )

    def direct_copy(j, flip):
        to = core if flip == 0 else 1 - core
        return pltpu.make_async_remote_copy(
            src_ref=pbuf.at[j, to, lax.rem(x + 1, n_x), :, sizes[j]],
            dst_ref=xbuf.at[j, flip, :, sizes[j]],
            send_sem=usend.at[j, flip],
            recv_sem=urecv.at[j, flip],
            device_id={"tp": lax.rem(x + 1, n_x) * 2 + to},
            device_id_type=MESH,
        )

    def detour_copy(j):
        return pltpu.make_async_remote_copy(
            src_ref=sbuf.at[j, 0, :, sizes[j]],
            dst_ref=detour.at[detours.index(j), :, sizes[j]],
            send_sem=xsend.at[j, 0],
            recv_sem=rrecv.at[detours.index(j)],
            device_id={"sp": inner, "tp": across},
            device_id_type=MESH,
        )

    def detour_end_copy(j):
        return pltpu.make_async_remote_copy(
            src_ref=detour.at[detours.index(j), :, sizes[j]],
            dst_ref=rbuf.at[j, 0, :, sizes[j]],
            send_sem=rsend.at[detours.index(j)],
            recv_sem=xrecv.at[j, 0],
            device_id={"sp": outer},
            device_id_type=MESH,
        )

    def pass_on(j):
        pair_copy(j).wait_recv()
        for dx in range(1, n_x):
            other = lax.rem(x + dx, n_x)
            both = pbuf[j, core, other, :, sizes[j]].astype(F32) + dbuf[j, other, :, sizes[j]].astype(F32)
            sbuf[j, dx - 1, :, sizes[j]] = both.astype(BF16)
            if j in detours:
                @pl.when(at_end)
                def _():
                    detour_copy(j).start()

                @pl.when(jnp.logical_not(at_end))
                def _():
                    cross_copy(j, dx).start()
            else:
                cross_copy(j, dx).start()
        own[j, :, sizes[j]] = pbuf[j, core, x, :, sizes[j]].astype(F32) + dbuf[j, x, :, sizes[j]].astype(F32)

    def project(j):
        part = proj[:, spans[j]] + jnp.dot(attn[:, heads_width:], gw[:, spans[j]], preferred_element_type=F32)
        for b in range(n_tp):
            pbuf[j, b % 2, b // 2, :, sizes[j]] = part[b * out_rows : (b + 1) * out_rows].astype(BF16)
        if j < direct:
            direct_pair_copy(j).start()
            for c in range(2):
                direct_copy(j, c).start()
        else:
            pair_copy(j).start()

    for j in range(direct + 1):
        project(j)
    project(direct + 1)
    pass_on(direct)
    for j in range(direct + 2, chunks):
        project(j)
        if j > direct + 2:
            pass_on(j - 2)
    for j in range(chunks - 2, chunks):
        pass_on(j)

    for j in detours:
        @pl.when(beside_end)
        def _():
            detour_copy(j).wait_recv()
            detour_end_copy(j).start()

    for j in range(direct):
        direct_pair_copy(j).wait()
        for c in range(2):
            direct_copy(j, c).wait()
        value = pbuf[j, core, x, :, sizes[j]].astype(F32) + dbuf[j, x, :, sizes[j]].astype(F32)
        for c in range(2):
            value = value + xbuf[j, c, :, sizes[j]].astype(F32)
        out_ref[:, spans[j]] = value.astype(BF16)
    for j in range(direct, chunks):
        value = own[j, :, sizes[j]]
        for dx in range(1, n_x):
            cross_copy(j, dx).wait_recv()
            value = value + rbuf[j, dx - 1, :, sizes[j]].astype(F32)
        out_ref[:, spans[j]] = value.astype(BF16)

    for j in range(direct, chunks):
        pair_copy(j).wait_send()
        for dx in range(1, n_x):
            cross_copy(j, dx).wait_send()
    for j in detours:
        @pl.when(beside_end)
        def _():
            detour_end_copy(j).wait_send()

    @pl.when(has_right)
    def _():
        halo_copy(0).wait_send()

    @pl.when(has_left)
    def _():
        halo_copy(1).wait_send()

    if lend:
        @pl.when(at_end)
        def _():
            lend_queries().wait_send()

        @pl.when(beside_end)
        def _():
            for copy in return_lent():
                copy.wait_send()

    def drain(source, carry):
        for g in range(kvh):
            right = has_right & (source <= me)
            left = has_left & (source >= me)
            if lend and g == last:
                right = right & jnp.logical_not((me == n - 2) & (source >= n - 3))
                left = left & jnp.logical_not((me == 1) & (source <= 2))
            for part in range(2):
                @pl.when(right)
                def _():
                    block_copy(source, g, part, 0).wait_send()

                @pl.when(left)
                def _():
                    block_copy(source, g, part, 1).wait_send()

        return carry

    lax.fori_loop(0, n, drain, 0)


def solution(mesh):
    n, n_tp = mesh.shape["sp"], mesh.shape["tp"]

    def per_device(wq, wk, wv, gq, gk, gv, sink, qgain, kgain, ww, gw):
        rows = wq.shape[0]
        kvh = wk.shape[1] // HEAD
        group = wq.shape[1] // wk.shape[1]
        model = ww.shape[1]
        chunks = 8
        width = model // chunks
        cuts = [(j * width, (j + 1) * width) for j in range(chunks)]
        direct = 0
        n_x = n_tp // 2
        out_rows = rows // n_tp
        heads_width = kvh * group * HEAD
        span = group * rows
        if n_tp == 4 and model % 4096 == 0:
            direct = 1
            edges = [0]
            for part in (1, 3, 4, 5, 4, 4, 4, 4, 3):
                edges.append(edges[-1] + part * model // 32)
            cuts = list(zip(edges[:-1], edges[1:]))
            width = max(end - begin for begin, end in cuts)
        chunks = len(cuts)
        any_spec = pl.BlockSpec(memory_space=pl.ANY)
        vmem = pl.BlockSpec(memory_space=pltpu.VMEM)
        cross = max(n_x - 1, 1)
        lend = LEND and n >= 4 and kvh >= 2
        detours = (3,) if n >= 4 and n_x == 2 else ()
        return pl.pallas_call(
            functools.partial(kernel, n, n_tp, rows, kvh, group, cuts, direct, detours, lend),
            out_shape=pltpu.VMEM((out_rows, model), BF16),
            in_specs=[any_spec] * 11,
            out_specs=vmem,
            scratch_shapes=[
                pltpu.SMEM(sink.shape, F32),
                pltpu.VMEM((1, HEAD), F32),
                pltpu.VMEM((1, HEAD), F32),
                pltpu.VMEM((kvh, span, HEAD), BF16),
                pltpu.VMEM((kvh, 2, rows + 2 * WINDOW, HEAD), BF16),
                pltpu.VMEM((kvh, span, HEAD), BF16),
                pltpu.VMEM((kvh, rows, HEAD), BF16),
                pltpu.VMEM((kvh + lend, span, HEAD), BF16),
                pltpu.VMEM((n, kvh, 2, rows, HEAD), BF16),
                pltpu.VMEM(ww.shape, BF16),
                pltpu.VMEM(gw.shape, BF16),
                pltpu.VMEM((rows, HEAD), F32),
                pltpu.VMEM((rows, HEAD), F32),
                pltpu.VMEM((kvh + lend, 1, span), F32),
                pltpu.VMEM((kvh + lend, 1, span), F32),
                pltpu.VMEM((kvh + lend, HEAD, span), F32),
                pltpu.VMEM((rows, 2 * heads_width), BF16),
                pltpu.VMEM((rows, model), F32),
                pltpu.VMEM((chunks, 2, n_x, out_rows, width), BF16),
                pltpu.VMEM((chunks, n_x, out_rows, width), BF16),
                pltpu.VMEM((chunks, cross, out_rows, width), BF16),
                pltpu.VMEM((chunks, cross, out_rows, width), BF16),
                pltpu.VMEM((chunks, out_rows, width), F32),
                pltpu.VMEM((max(len(detours), 1), out_rows, width), BF16),
                pltpu.VMEM((HEAD, span), BF16),
                pltpu.VMEM((2, 1, span), F32),
                pltpu.VMEM((max(direct, 1), 2, out_rows, width), BF16),
                pltpu.VMEM((rows + 2 * WINDOW, span), F32),
                pltpu.SemaphoreType.DMA((4 * kvh + 2 * kvh * group + 5,)),
                pltpu.SemaphoreType.DMA((2, n, kvh, 2)),
                pltpu.SemaphoreType.DMA((n, kvh, 2)),
                pltpu.SemaphoreType.DMA((2,)),
                pltpu.SemaphoreType.DMA((2,)),
                pltpu.SemaphoreType.DMA((chunks,)),
                pltpu.SemaphoreType.DMA((chunks,)),
                pltpu.SemaphoreType.DMA((chunks, cross)),
                pltpu.SemaphoreType.DMA((chunks, cross)),
                pltpu.SemaphoreType.DMA((max(len(detours), 1),)),
                pltpu.SemaphoreType.DMA((max(len(detours), 1),)),
                pltpu.SemaphoreType.DMA((3,)),
                pltpu.SemaphoreType.DMA((3,)),
                pltpu.SemaphoreType.DMA((max(direct, 1), 2)),
                pltpu.SemaphoreType.DMA((max(direct, 1), 2)),
            ],
            compiler_params=pltpu.CompilerParams(
                collective_id=0, has_side_effects=True, vmem_limit_bytes=60 * 1024 * 1024
            ),
            name="hybrid",
        )(wq, wk, wv, gq, gk, gv, sink, qgain.reshape(1, HEAD), kgain.reshape(1, HEAD), ww, gw)

    return jax.shard_map(
        per_device,
        mesh=mesh,
        in_specs=(P(("grp", "sp"), "tp"),) * 6 + (P("tp"), P(), P(), P("tp", None), P("tp", None)),
        out_specs=P(("grp", "sp", "tp"), None),
        check_vma=False,
    )
```
